512 devices in a mesh: ep: 32 (over z, core), tp: 16 (over y, x).
Axes of the slice: x: 4, y: 4, z: 16, core: 2. Of those that a mesh axis runs over, the one named last changes fastest.
Arguments:
- recurrence_queries: bfloat16 [16384, 2048], P('ep', 'tp'), may hold values from -6 to 6
- forget_preact: bfloat16 [16384, 2048], P('ep', 'tp')
- recurrence_values: bfloat16 [16384, 2048], P('ep', 'tp'), may hold values from -6 to 6
- output_gate_preact: bfloat16 [16384, 2048], P('ep', 'tp'), may hold values from -6 to 6
- forget_floor_logits: float32 [2048], P('tp')
- surge_log_decay: float32 [16384, 16], P('ep', 'tp'), may hold values from -0.7 to 0
- head_norm_gain: float32 [128], replicated, may hold values from 0.1 to 1.9
- recurrence_out_weight: bfloat16 [2048, 2048], P(None, 'tp'), may hold values from -0.125 to 0.125
- second_micro_rows: bfloat16 [4096, 2048], P('ep'), may hold values from -6 to 6
- expert_norm_gain: float32 [2048], replicated, may hold values from 0.1 to 1.9
- row_group_index: int32 [4096], P('ep'), may hold values from 0 to 3, as said below
- group_expert_index: int32 [4096, 2], P('ep'), may hold values from 0 to 7, as said below
- chosen_expert_weight: float32 [4096, 2], P('ep'), may hold values from 0.2 to 1
- expert_gate_weight: bfloat16 [32, 2048, 4096], P('ep', None, 'tp'), may hold values from -0.125 to 0.125
- expert_up_weight: bfloat16 [32, 2048, 4096], P('ep', None, 'tp'), may hold values from -0.125 to 0.125
- expert_down_weight: bfloat16 [32, 4096, 2048], P('ep', None, 'tp'), may hold values from -0.09375 to 0.09375
Outputs:
- mixed: bfloat16 [16384, 2048], P('ep', 'tp')
- expert_out: bfloat16 [4096, 2048], P('ep', 'tp')
The draws below stay inside these ranges and needn't reach their ends.
Inputs may be any that keep to these rules, and one draw needn't show every extreme that they name: group_expert_index names two different experts of the row's group; the expert's number is row_group_index * 8 + group_expert_index. Among the rows of one index of ep no expert is named more than 12 times, and some expert exactly 12 times. `group_expert_index`: the two entries of a row differ.
All inputs are finite; a program needn't handle non-finite values.
Results may differ from the reference program's by a relative error of at most 0.009.
Values may be sent and summed in bfloat16 or wider, within the bound.
A program may use at most 64 MiB of HBM per device.

```python
import math
import jax
import jax.numpy as jnp
from jax import lax

D = 2048
HEADS = 16
KEY_DIM = 128
VAL_DIM = 128
BLOCK = 64
EXPERTS = 32
GROUPS = 4
FF = 4096
TOK_M = 512
LENGTH = 16384
EXP_ROWS = 128
ALL_ROWS = 4096
CAP = 12
N_EP = 32


def draw_forget_preact(key, part):
    array_shape = (LENGTH, HEADS * KEY_DIM)
    base = jax.random.normal(jax.random.fold_in(key, 1), array_shape, jnp.float32)
    shift = jax.random.uniform(jax.random.fold_in(key, 2), (LENGTH // TOK_M, 1), jnp.float32, -1.5, 1.5)
    return (base + jnp.repeat(shift, TOK_M, axis=0)).astype(jnp.bfloat16)


def draw_forget_floor_logits(key, part):
    share = 0.5
    slow = jax.random.uniform(jax.random.fold_in(key, 21), (HEADS, 1), jnp.float32) < share
    spread = jax.random.uniform(jax.random.fold_in(key, 22), (HEADS, KEY_DIM), jnp.float32, 0.5, 2.0) / LENGTH
    quick = jnp.exp(jax.random.uniform(jax.random.fold_in(key, 23), (HEADS, KEY_DIM), jnp.float32, math.log(0.02), math.log(0.066)))
    rate = jnp.where(slow, spread, quick)
    return jnp.log((1.0 - rate) / rate).reshape(-1).astype(jnp.float32)


def draw_surge_log_decay(key, part):
    hit = jax.random.uniform(jax.random.fold_in(key, 31), (LENGTH, HEADS), jnp.float32) < 6.0 / LENGTH
    depth = jnp.log(jax.random.uniform(jax.random.fold_in(key, 32), (LENGTH, HEADS), jnp.float32, 0.5, 0.8))
    return jnp.where(hit, depth, 0.0).astype(jnp.float32)


def route_parts(key):
    block_total = ALL_ROWS // EXP_ROWS
    unit_rows = EXP_ROWS // 32
    patterns = jnp.array([[12, 8, 6, 6], [12, 10, 6, 4]], jnp.int32) * unit_rows
    chosen = jax.random.randint(jax.random.fold_in(key, 11), (block_total,), 0, 2)

    def one_block(index):
        sub_key = jax.random.fold_in(key, 100 + index)
        counts = patterns[chosen[index]]
        counts = counts[jax.random.permutation(jax.random.fold_in(sub_key, 1), 4)]
        bounds = jnp.cumsum(counts)
        position = jnp.arange(EXP_ROWS, dtype=jnp.int32)
        group = jnp.sum((position[:, None] >= bounds[None, :]).astype(jnp.int32), axis=1)
        begins = bounds - counts
        within = position - begins[group]
        orders = jnp.stack([jax.random.permutation(jax.random.fold_in(sub_key, 2 + g), 8) for g in range(4)])
        first = orders[group, within % 8]
        second = orders[group, (within + 4) % 8]
        row_perm = jax.random.permutation(jax.random.fold_in(sub_key, 9), EXP_ROWS)
        inverse = jnp.argsort(row_perm)
        return (group[inverse], jnp.stack([first, second], axis=1)[inverse])
    groups, local_sets = jax.vmap(one_block)(jnp.arange(block_total))
    return (groups.reshape(-1).astype(jnp.int32), local_sets.reshape(-1, 2).astype(jnp.int32))


def draw_row_group_index(key, part):
    return route_parts(jax.random.fold_in(key, 7))[0]


def draw_group_expert_index(key, part):
    return route_parts(jax.random.fold_in(key, 7))[1]


def block_scale(own_key, dims, split, low, largest):
    factor_of, own = 1.0, jax.random.fold_in(own_key, 6)
    for axis_at, shards_of in split:
        draws = jnp.exp(jax.random.uniform(jax.random.fold_in(own, axis_at), (shards_of,), jnp.float32, low / len(split), largest / len(split)))
        factor_of = factor_of * jnp.repeat(draws, dims[axis_at] // shards_of).reshape([-1 if axis == axis_at else 1 for axis in range(len(dims))])
    return factor_of


def bell_draw(key, dims, scale, reach, shards=(), kind=jnp.bfloat16):
    result = scale * jax.random.normal(key, dims, jnp.float32)
    if shards:
        result = result * block_scale(key, dims, shards, -0.22, 0.18)
    return jnp.clip(result, -reach, reach).astype(kind)


def setup_inputs(seed: int = 0) -> dict:
    splits = jax.random.split(jax.random.key(seed), 17)
    return {
        "recurrence_queries": bell_draw(splits[0], (LENGTH, HEADS * KEY_DIM), 1.0, 6.0, ((0, 32), (1, 16))),
        "forget_preact": draw_forget_preact(jax.random.fold_in(splits[16], 71), 0),
        "recurrence_values": bell_draw(splits[2], (LENGTH, HEADS * VAL_DIM), 1.0, 6.0, ((0, 32), (1, 16))),
        "output_gate_preact": bell_draw(splits[3], (LENGTH, HEADS * VAL_DIM), 1.0, 6.0, ((0, 32), (1, 16))),
        "forget_floor_logits": draw_forget_floor_logits(jax.random.fold_in(splits[16], 71), 0),
        "surge_log_decay": draw_surge_log_decay(jax.random.fold_in(splits[16], 71), 0),
        "head_norm_gain": jnp.clip(1.0 + 0.18 * jax.random.normal(splits[6], (VAL_DIM,), jnp.float32), 0.1, 1.9),
        "recurrence_out_weight": bell_draw(splits[7], (HEADS * VAL_DIM, D), (HEADS * VAL_DIM) ** -0.5, 0.125, ((1, 16),)),
        "second_micro_rows": bell_draw(splits[8], (ALL_ROWS, D), 1.0, 6.0, ((0, 32),)),
        "expert_norm_gain": jnp.clip(1.0 + 0.18 * jax.random.normal(splits[9], (D,), jnp.float32), 0.1, 1.9),
        "row_group_index": draw_row_group_index(jax.random.fold_in(splits[16], 71), 0),
        "group_expert_index": draw_group_expert_index(jax.random.fold_in(splits[16], 71), 0),
        "chosen_expert_weight": jnp.clip(0.2 + 0.8 * jax.random.uniform(splits[12], (ALL_ROWS, 2), jnp.float32) ** block_scale(splits[12], (ALL_ROWS, 2), ((0, 32),), -0.2, 0.2), 0.2, 1.0),
        "expert_gate_weight": bell_draw(splits[13], (EXPERTS, D, FF), D ** -0.5, 0.125, ((0, 32), (2, 16))),
        "expert_up_weight": bell_draw(splits[14], (EXPERTS, D, FF), D ** -0.5, 0.125, ((0, 32), (2, 16))),
        "expert_down_weight": bell_draw(splits[15], (EXPERTS, FF, D), FF ** -0.5, 0.09375, ((0, 32), (2, 16))),
    }


NORM_EPS = 1e-06
EXACT_PRECISION = lax.Precision.HIGHEST

def block_recurrence(query_activated, key_in, value_act, forget_log_value, state_init):
    block_len = query_activated.shape[1]
    causal = (jnp.arange(block_len)[:, None] >= jnp.arange(block_len)[None, :])[:, :, None, None]

    def block_step(current_state, block_inputs):
        query_tile, key_tile, value_tile, g_block = block_inputs
        running_total_sum = jnp.cumsum(g_block, axis=0)
        state_carried_out = jnp.einsum('cra,ran->crn', query_tile * jnp.exp(running_total_sum), current_state, precision=EXACT_PRECISION)
        relative = jnp.where(causal, running_total_sum[:, None] - running_total_sum[None, :], 0.0)
        decays = jnp.where(causal, jnp.exp(relative), 0.0)
        scores = jnp.einsum('thk,tshk,shk->hts', query_tile, decays, key_tile, precision=EXACT_PRECISION)
        output = state_carried_out + jnp.einsum('hts,shv->thv', scores, value_tile, precision=EXACT_PRECISION)
        final_log_value = running_total_sum[-1]
        current_state = jnp.exp(final_log_value)[:, :, None] * current_state + jnp.einsum('ceu,cex->eux', key_tile * jnp.exp(final_log_value[None] - running_total_sum), value_tile, precision=EXACT_PRECISION)
        return (current_state, output)
    return lax.scan(block_step, state_init, (query_activated, key_in, value_act, forget_log_value))

def token_mixing_layer(recurrence_queries, forget_preact, recurrence_values, output_gate_preact, forget_floor_logits, surge_log_decay, head_norm_gain, recurrence_out_weight):
    sequence_length = recurrence_queries.shape[0]
    number_of_heads = surge_log_decay.shape[1]
    key_feature_width = recurrence_queries.shape[1] // number_of_heads
    val_dim = recurrence_values.shape[1] // number_of_heads
    rate = jax.nn.sigmoid(-forget_floor_logits)
    input_gate_value = rate * jax.nn.sigmoid(-forget_preact.astype(jnp.float32))
    forget_log_value = jnp.log1p(-input_gate_value).reshape(sequence_length, number_of_heads, key_feature_width) + surge_log_decay[:, :, None]
    query_activated = jax.nn.silu(recurrence_queries.astype(jnp.float32)).reshape(sequence_length, number_of_heads, key_feature_width)
    key_in = input_gate_value.reshape(sequence_length, number_of_heads, key_feature_width)
    value_act = recurrence_values.astype(jnp.float32).reshape(sequence_length, number_of_heads, val_dim)
    block_count = sequence_length // BLOCK

    def to_blocks(array):
        return array.reshape(block_count, BLOCK, number_of_heads, array.shape[-1])
    state_init = jnp.zeros((number_of_heads, key_feature_width, val_dim), jnp.float32)
    _, recur_out = block_recurrence(to_blocks(query_activated), to_blocks(key_in), to_blocks(value_act), to_blocks(forget_log_value), state_init)
    recur_out = recur_out.reshape(sequence_length, number_of_heads, val_dim)
    normed = recur_out * lax.rsqrt(lax.optimization_barrier(jnp.mean(recur_out * recur_out, axis=-1, keepdims=True)) + NORM_EPS) * head_norm_gain
    gate_act = jax.nn.silu(output_gate_preact.astype(jnp.float32)).reshape(sequence_length, number_of_heads, val_dim)
    gated_heads = (normed * gate_act).reshape(sequence_length, number_of_heads * val_dim).astype(jnp.bfloat16)
    return jnp.dot(gated_heads, recurrence_out_weight, preferred_element_type=jnp.float32).astype(jnp.bfloat16)

def routed_experts(second_micro_rows, expert_norm_gain, row_group_index, group_expert_index, chosen_expert_weight, expert_gate_weight, expert_up_weight, expert_down_weight):
    row_count = second_micro_rows.shape[0]
    model_width = second_micro_rows.shape[1]
    expert_count = expert_gate_weight.shape[0]
    per_group = expert_count // GROUPS
    rows_float = second_micro_rows.astype(jnp.float32)
    normed_rows = (rows_float * lax.rsqrt(lax.optimization_barrier(jnp.mean(rows_float * rows_float, axis=-1, keepdims=True)) + NORM_EPS) * expert_norm_gain).astype(jnp.bfloat16)
    expert_choice = (row_group_index[:, None] * per_group + group_expert_index).astype(jnp.int32)
    flat_expert = expert_choice.reshape(-1)
    onehot = (flat_expert[:, None] == jnp.arange(expert_count, dtype=jnp.int32)[None, :]).astype(jnp.int32)
    rank_index = lax.optimization_barrier(jnp.sum((jnp.cumsum(onehot, axis=0) - onehot) * onehot, axis=1)).astype(jnp.int32)
    room_size = N_EP * CAP
    slot_index = (flat_expert * room_size + rank_index).astype(jnp.int32)
    owner_row = jnp.full((expert_count * room_size,), row_count, jnp.int32).at[slot_index].set((jnp.arange(2 * row_count) // 2).astype(jnp.int32))
    padded = jnp.concatenate([normed_rows, jnp.zeros((1, model_width), jnp.bfloat16)], axis=0)

    def expert_block(operands):
        row_index, gate_mat, up_mat, down_mat = operands
        gathered_rows = padded[row_index]
        gate_act = jnp.dot(gathered_rows, gate_mat, preferred_element_type=jnp.float32)
        up_act = jnp.dot(gathered_rows, up_mat, preferred_element_type=jnp.float32)
        expert_hidden = (jax.nn.silu(gate_act) * up_act).astype(jnp.bfloat16)
        return jnp.dot(expert_hidden, down_mat, preferred_element_type=jnp.float32).astype(jnp.bfloat16)
    expert_result = lax.map(expert_block, (owner_row.reshape(expert_count, room_size), expert_gate_weight, expert_up_weight, expert_down_weight))
    picked = expert_result.reshape(expert_count * room_size, model_width)[slot_index]
    picked = picked.reshape(row_count, 2, model_width).astype(jnp.float32)
    return lax.optimization_barrier(jnp.sum(picked * chosen_expert_weight[:, :, None], axis=1)).astype(jnp.bfloat16)

def reference(recurrence_queries, forget_preact, recurrence_values, output_gate_preact, forget_floor_logits, surge_log_decay, head_norm_gain, recurrence_out_weight, second_micro_rows, expert_norm_gain, row_group_index, group_expert_index, chosen_expert_weight, expert_gate_weight, expert_up_weight, expert_down_weight):
    mixed = token_mixing_layer(recurrence_queries, forget_preact, recurrence_values, output_gate_preact, forget_floor_logits, surge_log_decay, head_norm_gain, recurrence_out_weight)
    expert_out = routed_experts(second_micro_rows, expert_norm_gain, row_group_index, group_expert_index, chosen_expert_weight, expert_gate_weight, expert_up_weight, expert_down_weight)
    return (mixed, expert_out)
```

```python
import functools

import jax
import jax.numpy as jnp
from jax import lax
from jax.experimental import pallas as pl
from jax.experimental.pallas import tpu as pltpu
from jax.sharding import PartitionSpec as P

MESH = pl.DeviceIdType.MESH
F32, BF16 = jnp.float32, jnp.bfloat16
EPS = 1e-06
GROUPS = 4
CAP = 12
SLOT = 16
SIDE = 4
NT = (((1,), (1,)), ((), ()))
OFFSETS = (0, -1, 1, 2)


def silu(v):
    return v / (1.0 + jnp.exp(-v))


class Gather:
    def __init__(self, buf, send, recv, ep, y, x):
        self.buf, self.send, self.recv, self.ep, self.y, self.x = buf, send, recv, ep, y, x
        self.rows = buf.shape[1]

    def tp(self, color, a, b):
        dy, dx = (b, a) if color == 0 else (a, b)
        return lax.rem(self.y + dy + SIDE, SIDE) * SIDE + lax.rem(self.x + dx + SIDE, SIDE)

    def span(self, color, part):
        half = self.rows // 2
        start = color * half
        if part == 1:
            return pl.ds(start, half // 2)
        if part == 2:
            return pl.ds(start + half // 2, half // 2)
        return pl.ds(start, half)

    def copy(self, color, slot, block, part, to):
        region = self.buf.at[self.tp(color, *block), self.span(color, part), :]
        return pltpu.make_async_remote_copy(
            src_ref=region,
            dst_ref=region,
            send_sem=self.send.at[color, slot],
            recv_sem=self.recv.at[color, slot],
            device_id=(self.ep, self.tp(color, *to)),
            device_id_type=MESH,
        )

    def out(self, slot):
        if slot < 4:
            return [((0, 0), 0, (1, 0)), ((0, 0), 0, (-1, 0)), ((-1, 0), 1, (1, 0)), ((1, 0), 2, (-1, 0))][slot]
        j, k = divmod(slot - 4, 4)
        a = OFFSETS[j]
        return [((a, 0), 0, (0, 1)), ((a, 0), 0, (0, -1)), ((a, -1), 1, (0, 1)), ((a, 1), 2, (0, -1))][k]

    def landed(self, slot):
        if slot < 4:
            return [((-1, 0), 0), ((1, 0), 0), ((2, 0), 1), ((2, 0), 2)][slot]
        j, k = divmod(slot - 4, 4)
        a = OFFSETS[j]
        return [((a, -1), 0), ((a, 1), 0), ((a, 2), 1), ((a, 2), 2)][k]

    def start(self, color, *slots):
        for slot in slots:
            self.copy(color, slot, *self.out(slot)).start()

    def arrive(self, color, *slots):
        for slot in slots:
            block, part = self.landed(slot)
            self.copy(color, slot, block, part, (1, 0)).wait_recv()

    def begin(self):
        for color in (0, 1):
            self.start(color, 0, 1, 4, 5)

    def relay(self):
        for k in (0, 1):
            for color in (0, 1):
                self.arrive(color, k)
                self.start(color, 2 + k, 4 + 4 * (k + 1), 5 + 4 * (k + 1))
        for color in (0, 1):
            self.arrive(color, 4)
            self.start(color, 6)
            self.arrive(color, 5)
            self.start(color, 7)
        for color in (0, 1):
            self.arrive(color, 2, 3)
            self.start(color, 16, 17)
        for j in (1, 2, 3):
            for color in (0, 1):
                self.arrive(color, 4 + 4 * j)
                self.start(color, 6 + 4 * j)
                self.arrive(color, 5 + 4 * j)
                self.start(color, 7 + 4 * j)
        for j in (0, 1, 2, 3):
            for color in (0, 1):
                self.arrive(color, 6 + 4 * j, 7 + 4 * j)

    def drain(self):
        for color in (0, 1):
            for slot in range(20):
                self.copy(color, slot, *self.out(slot)).wait_send()


def exchange_copy(src, dst, send, recv, peer, mine, tp):
    return pltpu.make_async_remote_copy(
        src_ref=src,
        dst_ref=dst,
        send_sem=send.at[peer],
        recv_sem=recv.at[mine],
        device_id=(peer, tp),
        device_id_type=MESH,
    )


def kernel(
    n_ep,
    q_hbm, fp_hbm, v_hbm, og_hbm, floor_ref, surge_ref, gain_ref, wout_hbm,
    rows_hbm, ngain_ref, grp_ref, gex_ref, cw_ref, wg_hbm, wu_hbm, wd_hbm,
    mixed_ref, eout_ref,
    q_b, fp_b, v_b, og_b, rows_b, wout_b, wg_b, wu_b, wd_b, in_sem,
    outgo, arrived, result, returned, weights,
    xbuf, hbuf, mbuf,
    cum, keyin, qact, qdec, local_out,
    state, slices, decays, own_decay, prefix, incoming,
    d_send, d_recv, c_send, c_recv,
    s_send, s_recv, e_send, e_recv, p_send, p_recv,
    x_send, x_recv, h_send, h_recv, m_send, m_recv,
):
    me, tp = lax.axis_index("ep"), lax.axis_index("tp")
    y, x = lax.div(tp, SIDE), lax.rem(tp, SIDE)
    n_serve = n_ep // 2
    serving = lax.rem(me, 2) == 1
    share = lax.div(me, 2)

    barrier = pltpu.get_barrier_semaphore()

    @pl.loop(1, n_ep)
    def _(d):
        pl.semaphore_signal(barrier, inc=1, device_id=(lax.rem(me + d, n_ep), tp), device_id_type=MESH)

    for dy, dx in ((0, 1), (0, -1), (1, 0), (-1, 0)):
        other = lax.rem(y + dy + SIDE, SIDE) * SIDE + lax.rem(x + dx + SIDE, SIDE)
        pl.semaphore_signal(barrier, inc=1, device_id=(me, other), device_id_type=MESH)

    loads = {}
    for k, (name, src, dst) in enumerate(
        (
            ("rows", rows_hbm, rows_b), ("fp", fp_hbm, fp_b), ("q", q_hbm, q_b), ("v", v_hbm, v_b),
            ("og", og_hbm, og_b), ("wg", wg_hbm.at[0], wg_b), ("wu", wu_hbm.at[0], wu_b),
            ("wd", wd_hbm.at[0], wd_b), ("wout", wout_hbm, wout_b),
        )
    ):
        loads[name] = pltpu.make_async_copy(src, dst, in_sem.at[k])
        loads[name].start()

    count = grp_ref.shape[1]
    per_group = n_ep // GROUPS
    ex0 = grp_ref[...] * per_group + gex_ref[0:1, :]
    ex1 = grp_ref[...] * per_group + gex_ref[1:2, :]
    e_iota = lax.broadcasted_iota(jnp.int32, (n_ep, count), 0)
    hit0, hit1 = (e_iota == ex0).astype(F32), (e_iota == ex1).astype(F32)
    before = lax.broadcasted_iota(jnp.int32, (count, count), 0) < lax.broadcasted_iota(jnp.int32, (count, count), 1)
    earlier = jnp.dot((hit0 + hit1).astype(BF16), before.astype(F32).astype(BF16), preferred_element_type=F32)
    slot0 = ex0 * SLOT + jnp.sum(earlier * hit0, axis=0, keepdims=True).astype(jnp.int32)
    slot1 = ex1 * SLOT + jnp.sum(earlier * hit1, axis=0, keepdims=True).astype(jnp.int32)
    s_iota = lax.broadcasted_iota(jnp.int32, (n_ep * SLOT, count), 0)
    at0, at1 = s_iota == slot0, s_iota == slot1
    chosen = jnp.where(at0, cw_ref[0:1, :], 0.0) + jnp.where(at1, cw_ref[1:2, :], 0.0)
    turned = chosen.T
    high = turned.astype(BF16)
    weights[0] = high
    weights[1] = (turned - high.astype(F32)).astype(BF16)
    place = jnp.where(at0 | at1, 1.0, 0.0).astype(BF16)

    loads["rows"].wait()
    columns = pl.ds(pl.multiple_of(tp * 128, 128), 128)
    square = jnp.zeros((count, 128), F32)
    for k in range(rows_b.shape[1] // 128):
        part = rows_b[:, k * 128 : (k + 1) * 128].astype(F32)
        square = square + part * part
    scale = lax.rsqrt(jnp.sum(square, axis=1, keepdims=True) * (1.0 / rows_b.shape[1]) + EPS)
    normed = (rows_b[:, columns].astype(F32) * scale * ngain_ref[:, columns]).astype(BF16)
    outgo[...] = jnp.dot(place, normed, preferred_element_type=F32).astype(BF16).reshape(outgo.shape)

    pl.semaphore_wait(barrier, n_ep - 1 + 4)

    @pl.loop(1, n_ep)
    def _(d):
        peer = lax.rem(me + d, n_ep)
        exchange_copy(outgo.at[peer], arrived.at[me], d_send, d_recv, peer, me, tp).start()

    loads["fp"].wait()
    loads["q"].wait()
    loads["v"].wait()
    length = fp_b.shape[0]
    rate = jax.nn.sigmoid(-floor_ref[...])
    lower = lax.broadcasted_iota(jnp.int32, (128, 128), 0) >= lax.broadcasted_iota(jnp.int32, (128, 128), 1)
    lower = jnp.where(lower, 1.0, 0.0)
    carry = jnp.zeros((1, 128), F32)
    for b in range(length // 128):
        r = slice(b * 128, b * 128 + 128)
        gate = rate * jax.nn.sigmoid(-fp_b[r, :].astype(F32))
        keyin[r, :] = gate
        total = jnp.dot(lower, jnp.log1p(-gate), precision=lax.Precision.HIGHEST, preferred_element_type=F32)
        total = total + jnp.sum(lower * surge_ref[b : b + 1, :], axis=1, keepdims=True) + carry
        cum[r, :] = total
        carry = total[127:128, :]
        qact[r, :] = silu(q_b[r, :].astype(F32))

    own_decay[0] = jnp.exp(carry)
    tail = jnp.exp(carry - cum[...]) * keyin[...]
    state[...] = jnp.dot(v_b[...].astype(F32).T.astype(BF16), tail.astype(BF16), preferred_element_type=F32).reshape(
        state.shape
    )

    @pl.loop(0, n_serve)
    def _(k):
        peer = 2 * k + 1

        @pl.when(peer != me)
        def _():
            exchange_copy(state.at[k], slices.at[me], s_send, s_recv, peer, me, tp).start()
            exchange_copy(own_decay.at[0], decays.at[me], e_send, e_recv, peer, me, tp).start()

    qdec[...] = (qact[...] * jnp.exp(cum[...])).astype(BF16)
    sub = 64

    @pl.loop(0, length // sub)
    def _(c):
        r = pl.ds(pl.multiple_of(c * sub, sub), sub)
        shape = (sub // 8, 8, 128)
        g, k, v = cum[r, :].reshape(shape), keyin[r, :].reshape(shape), v_b[r, :].astype(F32).reshape(shape)
        q = qact[r, :].reshape(shape)
        within = lax.broadcasted_iota(jnp.int32, (sub // 8, 8, 1), 1)
        total = jnp.sum(q * k, axis=2, keepdims=True) * v
        for d in range(1, 8):
            gd, kd, vd = (pltpu.roll(a, d, 1) for a in (g, k, v))
            w = jnp.sum(q * kd * jnp.exp(jnp.minimum(g - gd, 0.0)), axis=2, keepdims=True)
            total = total + jnp.where(within >= d, w, 0.0) * vd
        local_out[r, :] = total.reshape(sub, 128)

    half = length // 2
    t_iota = lax.broadcasted_iota(jnp.int32, (half, half), 0)
    u_iota = lax.broadcasted_iota(jnp.int32, (half, half), 1)
    for b in range(2):
        r = slice(b * half, (b + 1) * half)
        acc = jnp.zeros((half, half), F32)
        h = 8
        while h < half:
            g3 = cum[r, :].reshape(half // (2 * h), 2 * h, 128)
            fade = jnp.exp(-jnp.abs(g3 - g3[:, h - 1 : h, :])).reshape(half, 128)
            s = lax.dot_general(
                (qact[r, :] * fade).astype(BF16), (keyin[r, :] * fade).astype(BF16), NT, preferred_element_type=F32
            )
            pair = (t_iota // (2 * h) == u_iota // (2 * h)) & ((t_iota // h) % 2 == 1) & ((u_iota // h) % 2 == 0)
            acc = jnp.where(pair, s, acc)
            h *= 2
        local_out[r, :] += jnp.dot(acc.astype(BF16), v_b[r, :], preferred_element_type=F32)
    edge = cum[half - 1 : half, :]
    left, right = slice(0, half), slice(half, length)
    s = lax.dot_general(
        (qact[right, :] * jnp.exp(cum[right, :] - edge)).astype(BF16),
        (keyin[left, :] * jnp.exp(edge - cum[left, :])).astype(BF16),
        NT,
        preferred_element_type=F32,
    )
    local_out[right, :] += jnp.dot(s.astype(BF16), v_b[left, :], preferred_element_type=F32)

    @pl.when(serving)
    def _():
        slices[me] = state[share]
        decays[me] = own_decay[0]

        @pl.loop(1, n_ep)
        def _(d):
            peer = lax.rem(me + d, n_ep)
            exchange_copy(state.at[0], slices.at[peer], s_send, s_recv, me, peer, tp).wait_recv()
            exchange_copy(own_decay.at[0], decays.at[peer], e_send, e_recv, me, peer, tp).wait_recv()

        total = jnp.zeros(slices.shape[1:], F32)
        for k in range(n_ep):
            prefix[k] = total
            total = decays[k] * total + slices[k]

        @pl.loop(1, n_ep)
        def _(d):
            peer = lax.rem(me + d, n_ep)
            exchange_copy(prefix.at[peer], incoming.at[share], p_send, p_recv, peer, share, tp).start()

        incoming[share] = prefix[me]

    arrived[me] = outgo[me]

    @pl.loop(1, n_ep)
    def _(d):
        peer = lax.rem(me + d, n_ep)
        exchange_copy(outgo.at[peer], arrived.at[peer], d_send, d_recv, me, peer, tp).wait_recv()

    exp_rows = n_ep * CAP
    row = lax.broadcasted_iota(jnp.int32, (exp_rows, n_ep * SLOT), 0)
    col = lax.broadcasted_iota(jnp.int32, (exp_rows, n_ep * SLOT), 1)
    pack = jnp.where(row // CAP * SLOT + row % CAP == col, 1.0, 0.0).astype(BF16)
    xbuf[tp] = jnp.dot(pack, arrived[...].reshape(n_ep * SLOT, 128), preferred_element_type=F32).astype(BF16)
    gather_x = Gather(xbuf, x_send, x_recv, me, y, x)
    gather_h = Gather(hbuf, h_send, h_recv, me, y, x)
    gather_m = Gather(mbuf, m_send, m_recv, me, y, x)
    gather_x.begin()

    @pl.loop(0, n_serve)
    def _(k):
        @pl.when(2 * k + 1 != me)
        def _():
            exchange_copy(prefix.at[0], incoming.at[k], p_send, p_recv, me, k, tp).wait_recv()

    before_state = incoming[...].reshape(128, 128).astype(BF16)
    loads["og"].wait()
    out = local_out[...] + lax.dot_general(qdec[...], before_state, NT, preferred_element_type=F32)
    out = out * lax.rsqrt(jnp.mean(out * out, axis=1, keepdims=True) + EPS) * gain_ref[...]
    mbuf[tp] = (out * silu(og_b[...].astype(F32))).astype(BF16)

    gather_x.relay()
    loads["wg"].wait()
    loads["wu"].wait()
    tps = SIDE * SIDE
    feats = jnp.concatenate([xbuf[k] for k in range(tps)], axis=1)
    gate_act = jnp.dot(feats, wg_b[...], preferred_element_type=F32)
    up_act = jnp.dot(feats, wu_b[...], preferred_element_type=F32)
    hbuf[tp] = (silu(gate_act) * up_act).astype(BF16)
    gather_h.begin()
    gather_h.relay()
    gather_m.begin()
    loads["wd"].wait()
    hidden = jnp.concatenate([hbuf[k] for k in range(tps)], axis=1)
    res = jnp.dot(hidden, wd_b[...], preferred_element_type=F32).astype(BF16)
    row = lax.broadcasted_iota(jnp.int32, (n_ep * SLOT, exp_rows), 0)
    col = lax.broadcasted_iota(jnp.int32, (n_ep * SLOT, exp_rows), 1)
    spread = jnp.where((row // SLOT * CAP + row % SLOT == col) & (row % SLOT < CAP), 1.0, 0.0).astype(BF16)
    result[...] = jnp.dot(spread, res, preferred_element_type=F32).astype(BF16).reshape(result.shape)

    @pl.loop(1, n_ep)
    def _(d):
        peer = lax.rem(me + d, n_ep)
        exchange_copy(result.at[peer], returned.at[me], c_send, c_recv, peer, me, tp).start()

    returned[me] = result[me]
    gather_m.relay()
    loads["wout"].wait()
    heads = jnp.concatenate([mbuf[k] for k in range(tps)], axis=1)
    mixed_ref[...] = jnp.dot(heads, wout_b[...], preferred_element_type=F32).astype(BF16)

    @pl.loop(1, n_ep)
    def _(d):
        peer = lax.rem(me + d, n_ep)
        exchange_copy(result.at[peer], returned.at[peer], c_send, c_recv, me, peer, tp).wait_recv()

    back = returned[...].reshape(n_ep * SLOT, 128)
    eout_ref[...] = (
        jnp.dot(weights[0], back, preferred_element_type=F32) + jnp.dot(weights[1], back, preferred_element_type=F32)
    ).astype(BF16)

    @pl.loop(1, n_ep)
    def _(d):
        peer = lax.rem(me + d, n_ep)
        exchange_copy(outgo.at[peer], arrived.at[me], d_send, d_recv, peer, me, tp).wait_send()
        exchange_copy(result.at[peer], returned.at[me], c_send, c_recv, peer, me, tp).wait_send()

        @pl.when(serving)
        def _():
            exchange_copy(prefix.at[peer], incoming.at[share], p_send, p_recv, peer, share, tp).wait_send()

    @pl.loop(0, n_serve)
    def _(k):
        peer = 2 * k + 1

        @pl.when(peer != me)
        def _():
            exchange_copy(state.at[k], slices.at[me], s_send, s_recv, peer, me, tp).wait_send()
            exchange_copy(own_decay.at[0], decays.at[me], e_send, e_recv, peer, me, tp).wait_send()

    for gather in (gather_x, gather_h, gather_m):
        gather.drain()


def solution(mesh):
    n_ep, n_tp = mesh.shape["ep"], mesh.shape["tp"]

    def local(q, fp, v, og, floor, surge, gain, wout, rows, ngain, grp, gex, cw, wg, wu, wd):
        length, count = q.shape[0], rows.shape[0]
        hid, cols = wg.shape[2], wd.shape[2]
        exp_rows = n_ep * CAP
        vmem, anyspace = pl.BlockSpec(memory_space=pltpu.VMEM), pl.BlockSpec(memory_space=pl.ANY)
        dma = pltpu.SemaphoreType.DMA
        block = (n_ep, SLOT, 128)
        scratch = [
            pltpu.VMEM(q.shape, BF16), pltpu.VMEM(q.shape, BF16), pltpu.VMEM(q.shape, BF16), pltpu.VMEM(q.shape, BF16),
            pltpu.VMEM(rows.shape, BF16), pltpu.VMEM(wout.shape, BF16),
            pltpu.VMEM(wg.shape[1:], BF16), pltpu.VMEM(wu.shape[1:], BF16), pltpu.VMEM(wd.shape[1:], BF16),
            dma((9,)),
            pltpu.VMEM(block, BF16), pltpu.VMEM(block, BF16), pltpu.VMEM(block, BF16), pltpu.VMEM(block, BF16),
            pltpu.VMEM((2, count, n_ep * SLOT), BF16),
            pltpu.VMEM((n_tp, exp_rows, 128), BF16), pltpu.VMEM((n_tp, exp_rows, hid), BF16),
            pltpu.VMEM((n_tp, length, 128), BF16),
            pltpu.VMEM(q.shape, F32), pltpu.VMEM(q.shape, F32), pltpu.VMEM(q.shape, F32), pltpu.VMEM(q.shape, BF16),
            pltpu.VMEM(q.shape, F32),
            pltpu.VMEM((n_ep // 2, 256 // n_ep, 128), F32), pltpu.VMEM((n_ep, 256 // n_ep, 128), F32),
            pltpu.VMEM((n_ep, 1, 128), F32), pltpu.VMEM((1, 1, 128), F32),
            pltpu.VMEM((n_ep, 256 // n_ep, 128), F32), pltpu.VMEM((n_ep // 2, 256 // n_ep, 128), F32),
            dma((n_ep,)), dma((n_ep,)), dma((n_ep,)), dma((n_ep,)),
            dma((n_ep,)), dma((n_ep,)), dma((n_ep,)), dma((n_ep,)), dma((n_ep,)), dma((n_ep,)),
            dma((2, 20)), dma((2, 20)), dma((2, 20)), dma((2, 20)), dma((2, 20)), dma((2, 20)),
        ]
        return pl.pallas_call(
            functools.partial(kernel, n_ep),
            out_shape=(jax.ShapeDtypeStruct((length, cols), BF16), jax.ShapeDtypeStruct((count, cols), BF16)),
            in_specs=[anyspace] * 4 + [vmem] * 3 + [anyspace] * 2 + [vmem] * 4 + [anyspace] * 3,
            out_specs=(vmem, vmem),
            scratch_shapes=scratch,
            compiler_params=pltpu.CompilerParams(
                collective_id=0, has_side_effects=True, vmem_limit_bytes=60 * 1024 * 1024
            ),
        )(
            q, fp, v, og, floor.reshape(1, -1), surge.reshape(-1, 128), gain.reshape(1, -1), wout,
            rows, ngain.reshape(1, -1), grp.reshape(1, -1), gex.T, cw.T, wg, wu, wd,
        )

    return jax.shard_map(
        local,
        mesh=mesh,
        in_specs=(
            P("ep", "tp"), P("ep", "tp"), P("ep", "tp"), P("ep", "tp"), P("tp"), P("ep", "tp"), P(), P(None, "tp"),
            P("ep", None), P(), P("ep"), P("ep", None), P("ep", None),
            P("ep", None, "tp"), P("ep", None, "tp"), P("ep", None, "tp"),
        ),
        out_specs=(P("ep", "tp"), P("ep", "tp")),
        check_vma=False,
    )
```

```python
import functools

import jax
import jax.numpy as jnp
from jax import lax
from jax.experimental import pallas as pl
from jax.experimental.pallas import tpu as pltpu
from jax.sharding import PartitionSpec as P

MESH = pl.DeviceIdType.MESH
F32, BF16 = jnp.float32, jnp.bfloat16
EPS = 1e-06
GROUPS = 4
CAP = 12
SLOT = 16
SIDE = 4
NT = (((1,), (1,)), ((), ()))
OFFSETS = (0, -1, 1, 2)


def silu(v):
    return v / (1.0 + jnp.exp(-v))


class Gather:
    def __init__(self, buf, base, rows, send, recv, ep, y, x):
        self.buf, self.base, self.rows = buf, base, rows
        self.send, self.recv, self.ep, self.y, self.x = send, recv, ep, y, x

    def tp(self, color, a, b):
        dy, dx = (b, a) if color == 0 else (a, b)
        return lax.rem(self.y + dy + SIDE, SIDE) * SIDE + lax.rem(self.x + dx + SIDE, SIDE)

    def span(self, color, part):
        half = self.rows // 2
        start = self.base + color * half
        if part == 1:
            return pl.ds(start, half // 2)
        if part == 2:
            return pl.ds(start + half // 2, half // 2)
        return pl.ds(start, half)

    def copy(self, color, slot, block, part, to):
        region = self.buf.at[self.tp(color, *block), self.span(color, part), :]
        return pltpu.make_async_remote_copy(
            src_ref=region,
            dst_ref=region,
            send_sem=self.send.at[color, slot],
            recv_sem=self.recv.at[color, slot],
            device_id=(self.ep, self.tp(color, *to)),
            device_id_type=MESH,
        )

    def out(self, slot):
        if slot < 4:
            return [((0, 0), 0, (1, 0)), ((0, 0), 0, (-1, 0)), ((-1, 0), 1, (1, 0)), ((1, 0), 2, (-1, 0))][slot]
        j, k = divmod(slot - 4, 4)
        a = OFFSETS[j]
        return [((a, 0), 0, (0, 1)), ((a, 0), 0, (0, -1)), ((a, -1), 1, (0, 1)), ((a, 1), 2, (0, -1))][k]

    def landed(self, slot):
        if slot < 4:
            return [((-1, 0), 0), ((1, 0), 0), ((2, 0), 1), ((2, 0), 2)][slot]
        j, k = divmod(slot - 4, 4)
        a = OFFSETS[j]
        return [((a, -1), 0), ((a, 1), 0), ((a, 2), 1), ((a, 2), 2)][k]

    def start(self, color, *slots):
        for slot in slots:
            self.copy(color, slot, *self.out(slot)).start()

    def arrive(self, color, *slots):
        for slot in slots:
            block, part = self.landed(slot)
            self.copy(color, slot, block, part, (1, 0)).wait_recv()

    def begin(self):
        for color in (0, 1):
            self.start(color, 0, 1, 4, 5)

    def relay(self):
        self.relay_sends()
        self.relay_last()

    def relay_sends(self):
        self.relay_near()
        self.relay_far()

    def relay_near(self):
        self.relay_first()
        self.relay_second()

    def relay_first(self):
        for k in (0, 1):
            for color in (0, 1):
                self.arrive(color, k)
                self.start(color, 2 + k, 4 + 4 * (k + 1), 5 + 4 * (k + 1))

    def relay_second(self):
        for color in (0, 1):
            self.arrive(color, 4)
            self.start(color, 6)
            self.arrive(color, 5)
            self.start(color, 7)

    def relay_far(self):
        for color in (0, 1):
            self.arrive(color, 2, 3)
            self.start(color, 16, 17)
        for j in (1, 2, 3):
            for color in (0, 1):
                self.arrive(color, 4 + 4 * j)
                self.start(color, 6 + 4 * j)
                self.arrive(color, 5 + 4 * j)
                self.start(color, 7 + 4 * j)

    def relay_last(self):
        for j in (0, 1, 2, 3):
            for color in (0, 1):
                self.arrive(color, 6 + 4 * j, 7 + 4 * j)

    def drain(self):
        for color in (0, 1):
            for slot in range(20):
                self.copy(color, slot, *self.out(slot)).wait_send()


class Ring:
    def __init__(self, turn, send, recv, ep, y, x):
        self.turn, self.send, self.recv, self.ep, self.y, self.x = turn, send, recv, ep, y, x

    def pos(self, half, off=0):
        return lax.rem((self.x if half == self.turn else self.y) + off + SIDE, SIDE)

    def tp(self, half, off):
        if half == self.turn:
            return self.y * SIDE + self.pos(half, off)
        return self.pos(half, off) * SIDE + self.x

    def copy(self, half, slot, src, dst, off):
        return pltpu.make_async_remote_copy(
            src_ref=src,
            dst_ref=dst,
            send_sem=self.send.at[half, slot],
            recv_sem=self.recv.at[half, slot],
            device_id=(self.ep, self.tp(half, off)),
            device_id_type=MESH,
        )


def exchange_copy(src, dst, send, recv, peer, mine, tp):
    return pltpu.make_async_remote_copy(
        src_ref=src,
        dst_ref=dst,
        send_sem=send.at[peer],
        recv_sem=recv.at[mine],
        device_id=(peer, tp),
        device_id_type=MESH,
    )


def kernel(
    n_ep,
    q_hbm, fp_hbm, v_hbm, og_hbm, floor_hbm, surge_hbm, gain_hbm, wout_hbm,
    rows_hbm, ngain_hbm, grp_hbm, gex_hbm, cw_hbm, wg_hbm, wu_hbm, wd_hbm,
    mixed_hbm, eout_hbm,
    q_b, fp_b, v_b, og_b, floor_b, surge_b, gain_b, wout_b,
    rows_b, ngain_b, grp_b, gex_b, cw_b, wg_b, wu_b, wd_b, mixed_b, eout_b, in_sem, out_sem, own_sem,
    outgo, arrived, result, returned, weights, pack, spread,
    xbuf, hbuf, mbuf, wcross, staged, part, sums_out, sums_in,
    cum, keyin, qact, qdec, local_out,
    state, slices, decays, own_decay, prefix, incoming,
    d_send, d_recv, c_send, c_recv,
    s_send, s_recv, e_send, e_recv, p_send, p_recv,
    x_send, x_recv, h_send, h_recv, m_send, m_recv, w_send, w_recv, r_send, r_recv,
):
    me, tp = lax.axis_index("ep"), lax.axis_index("tp")
    y, x = lax.div(tp, SIDE), lax.rem(tp, SIDE)
    z, core = lax.div(me, 2), lax.rem(me, 2)
    n_z = n_ep // 2
    serving = core == 1

    loads = {}

    def load(*names):
        for name in names:
            loads[name].start()

    for k, (name, src, dst) in enumerate(
        (
            ("grp", grp_hbm, grp_b), ("gex", gex_hbm, gex_b), ("rows", rows_hbm, rows_b), ("ngain", ngain_hbm, ngain_b),
            ("wd", wd_hbm, wd_b), ("cw", cw_hbm, cw_b), ("floor", floor_hbm, floor_b), ("fp", fp_hbm, fp_b),
            ("surge", surge_hbm, surge_b), ("q", q_hbm, q_b), ("v", v_hbm, v_b), ("og", og_hbm, og_b),
            ("gain", gain_hbm, gain_b), ("wg", wg_hbm.at[0], wg_b), ("wu", wu_hbm.at[0], wu_b), ("wout", wout_hbm, wout_b),
        )
    ):
        loads[name] = pltpu.make_async_copy(src, dst, in_sem.at[k])
    load("grp", "gex", "rows", "ngain")

    barrier = pltpu.get_barrier_semaphore()
    for d in range(1, n_ep):
        pl.semaphore_signal(barrier, inc=1, device_id=(lax.rem(me + d, n_ep), tp), device_id_type=MESH)

    for dy, dx in ((0, 1), (0, -1), (1, 0), (-1, 0)):
        other = lax.rem(y + dy + SIDE, SIDE) * SIDE + lax.rem(x + dx + SIDE, SIDE)
        pl.semaphore_signal(barrier, inc=1, device_id=(me, other), device_id_type=MESH)

    load("wd", "floor", "fp", "surge", "q", "v", "cw", "og", "gain", "wg", "wu", "wout")

    loads["grp"].wait()
    loads["gex"].wait()
    count = grp_b.shape[1]
    per_group = n_ep // GROUPS
    ex0 = grp_b[...] * per_group + gex_b[0:1, :]
    ex1 = grp_b[...] * per_group + gex_b[1:2, :]
    e_iota = lax.broadcasted_iota(jnp.int32, (n_ep, count), 0)
    hit0, hit1 = (e_iota == ex0).astype(F32), (e_iota == ex1).astype(F32)
    before = lax.broadcasted_iota(jnp.int32, (count, count), 0) < lax.broadcasted_iota(jnp.int32, (count, count), 1)
    earlier = jnp.dot((hit0 + hit1).astype(BF16), before.astype(F32).astype(BF16), preferred_element_type=F32)
    slot0 = ex0 * SLOT + jnp.sum(earlier * hit0, axis=0, keepdims=True).astype(jnp.int32)
    slot1 = ex1 * SLOT + jnp.sum(earlier * hit1, axis=0, keepdims=True).astype(jnp.int32)
    s_iota = lax.broadcasted_iota(jnp.int32, (n_ep * SLOT, count), 0)
    at0, at1 = s_iota == slot0, s_iota == slot1
    place = jnp.where(at0 | at1, 1.0, 0.0).astype(BF16)

    loads["rows"].wait()
    loads["ngain"].wait()
    columns = pl.ds(pl.multiple_of(tp * 128, 128), 128)
    square = jnp.zeros((count, 128), F32)
    for k in range(rows_b.shape[1] // 128):
        piece = rows_b[:, k * 128 : (k + 1) * 128].astype(F32)
        square = square + piece * piece
    scale = lax.rsqrt(jnp.sum(square, axis=1, keepdims=True) * (1.0 / rows_b.shape[1]) + EPS)
    normed = (rows_b[:, columns].astype(F32) * scale * ngain_b[:, columns]).astype(BF16)
    outgo[...] = jnp.dot(place, normed, preferred_element_type=F32).astype(BF16).reshape(outgo.shape)

    pl.semaphore_wait(barrier, n_ep - 1 + 4)

    order = [(n_z // 2, c) for c in (1, 0)]
    for away in range(n_z // 2 - 1, 0, -1):
        order += [(way * away, c) for c in (1, 0) for way in (1, -1)]
    order.append((0, 0))
    peers = [lax.rem(z + away + n_z, n_z) * 2 + lax.rem(core + c + 1, 2) for away, c in order]

    def dispatch(peer):
        return exchange_copy(outgo.at[peer], arrived.at[me], d_send, d_recv, peer, me, tp)

    def give_back(peer):
        return exchange_copy(result.at[peer], returned.at[me], c_send, c_recv, peer, me, tp)

    for peer in peers:
        dispatch(peer).start()

    loads["wd"].wait()
    ring_g = Ring(0, h_send, h_recv, me, y, x)
    ring_w = Ring(1, w_send, w_recv, me, y, x)
    ring_r = Ring(1, r_send, r_recv, me, y, x)

    def cross(half, slot):
        mine = ring_w.pos(half)

        def to(off, part):
            there = ring_w.pos(half, off)
            return wd_b.at[there, part] if half == 0 else wd_b.at[part, there]

        whole, low, high = pl.ds(0, SIDE), pl.ds(0, SIDE // 2), pl.ds(SIDE // 2, SIDE // 2)
        src, dst = (
            (lambda: to(2, low), lambda: staged.at[half, 0]),
            (lambda: to(2, high), lambda: staged.at[half, 1]),
            (lambda: to(1, whole), lambda: wcross.at[half, mine]),
            (lambda: to(-1, whole), lambda: wcross.at[half, mine]),
            (lambda: staged.at[half, 0], lambda: wcross.at[half, ring_w.pos(half, -1), low]),
            (lambda: staged.at[half, 1], lambda: wcross.at[half, ring_w.pos(half, 1), high]),
        )[slot]
        return ring_w.copy(half, slot, src(), dst(), (1, -1)[slot % 2])

    def crossed(half, slot):
        low, high = pl.ds(0, SIDE // 2), pl.ds(SIDE // 2, SIDE // 2)
        region = (
            lambda: staged.at[half, 0],
            lambda: staged.at[half, 1],
            lambda: wcross.at[half, ring_w.pos(half, -1)],
            lambda: wcross.at[half, ring_w.pos(half, 1)],
            lambda: wcross.at[half, ring_w.pos(half, 2), low],
            lambda: wcross.at[half, ring_w.pos(half, 2), high],
        )[slot]()
        return ring_w.copy(half, slot, region, region, 1)

    for slot in range(4):
        for half in (0, 1):
            cross(half, slot).start()
    own_w = [
        pltpu.make_async_copy(wd_b.at[y], wcross.at[0, y], own_sem.at[0]),
        pltpu.make_async_copy(wd_b.at[:, x], wcross.at[1, x], own_sem.at[1]),
    ]
    for copy in own_w:
        copy.start()

    loads["floor"].wait()
    loads["fp"].wait()
    loads["surge"].wait()
    loads["q"].wait()
    loads["v"].wait()
    length = fp_b.shape[0]
    rate = jax.nn.sigmoid(-floor_b[...])
    lower = lax.broadcasted_iota(jnp.int32, (128, 128), 0) >= lax.broadcasted_iota(jnp.int32, (128, 128), 1)
    lower = jnp.where(lower, 1.0, 0.0)
    carry = jnp.zeros((1, 128), F32)
    for b in range(length // 128):
        r = slice(b * 128, b * 128 + 128)
        gate = rate * jax.nn.sigmoid(-fp_b[r, :].astype(F32))
        keyin[r, :] = gate
        total = jnp.dot(lower, jnp.log1p(-gate), precision=lax.Precision.HIGHEST, preferred_element_type=F32)
        total = total + jnp.sum(lower * surge_b[b : b + 1, :], axis=1, keepdims=True) + carry
        cum[r, :] = total
        carry = total[127:128, :]
        qact[r, :] = silu(q_b[r, :].astype(F32))

    own_decay[0] = jnp.exp(carry)
    tail = jnp.exp(carry - cum[...]) * keyin[...]
    state[...] = jnp.dot(v_b[...].astype(F32).T.astype(BF16), tail.astype(BF16), preferred_element_type=F32).reshape(
        state.shape
    )

    @pl.loop(0, n_z)
    def _(k):
        peer = 2 * k + 1

        @pl.when(peer != me)
        def _():
            exchange_copy(state.at[k], slices.at[me], s_send, s_recv, peer, me, tp).start()
            exchange_copy(own_decay.at[0], decays.at[me], e_send, e_recv, peer, me, tp).start()

    qdec[...] = (qact[...] * jnp.exp(cum[...])).astype(BF16)
    sub = 64

    @pl.loop(0, length // sub)
    def _(c):
        r = pl.ds(pl.multiple_of(c * sub, sub), sub)
        shape = (sub // 8, 8, 128)
        g, k, v = cum[r, :].reshape(shape), keyin[r, :].reshape(shape), v_b[r, :].astype(F32).reshape(shape)
        q = qact[r, :].reshape(shape)
        within = lax.broadcasted_iota(jnp.int32, (sub // 8, 8, 1), 1)
        total = jnp.sum(q * k, axis=2, keepdims=True) * v
        for d in range(1, 8):
            gd, kd, vd = (pltpu.roll(a, d, 1) for a in (g, k, v))
            w = jnp.sum(q * kd * jnp.exp(jnp.minimum(g - gd, 0.0)), axis=2, keepdims=True)
            total = total + jnp.where(within >= d, w, 0.0) * vd
        local_out[r, :] = total.reshape(sub, 128)

    half = length // 2
    t_iota = lax.broadcasted_iota(jnp.int32, (half, half), 0)
    u_iota = lax.broadcasted_iota(jnp.int32, (half, half), 1)
    for b in range(2):
        r = slice(b * half, (b + 1) * half)
        acc = jnp.zeros((half, half), F32)
        h = 8
        while h < half:
            g3 = cum[r, :].reshape(half // (2 * h), 2 * h, 128)
            fade = jnp.exp(-jnp.abs(g3 - g3[:, h - 1 : h, :])).reshape(half, 128)
            s = lax.dot_general(
                (qact[r, :] * fade).astype(BF16), (keyin[r, :] * fade).astype(BF16), NT, preferred_element_type=F32
            )
            pair = (t_iota // (2 * h) == u_iota // (2 * h)) & ((t_iota // h) % 2 == 1) & ((u_iota // h) % 2 == 0)
            acc = jnp.where(pair, s, acc)
            h *= 2
        local_out[r, :] += jnp.dot(acc.astype(BF16), v_b[r, :], preferred_element_type=F32)
    edge = cum[half - 1 : half, :]
    left, right = slice(0, half), slice(half, length)
    s = lax.dot_general(
        (qact[right, :] * jnp.exp(cum[right, :] - edge)).astype(BF16),
        (keyin[left, :] * jnp.exp(edge - cum[left, :])).astype(BF16),
        NT,
        preferred_element_type=F32,
    )
    local_out[right, :] += jnp.dot(s.astype(BF16), v_b[left, :], preferred_element_type=F32)

    part_rows, part_slots = n_z * CAP, n_z * SLOT

    def matches(shape, axis):
        r, s = lax.broadcasted_iota(jnp.int32, shape, axis), lax.broadcasted_iota(jnp.int32, shape, 1 - axis)
        return jnp.where(r // CAP * SLOT + r % CAP == s, 1.0, 0.0).astype(BF16)

    pack[...] = matches((part_rows, part_slots), 0)
    spread[...] = matches((part_slots, part_rows), 1)
    loads["cw"].wait()
    chosen = jnp.where(at0, cw_b[0:1, :], 0.0) + jnp.where(at1, cw_b[1:2, :], 0.0)
    turned = chosen.T
    high = turned.astype(BF16)
    weights[0] = high
    weights[1] = (turned - high.astype(F32)).astype(BF16)

    gather_x = Gather(xbuf, 0, 2 * part_rows, x_send, x_recv, me, y, x)
    gather_m = Gather(mbuf, 0, length, m_send, m_recv, me, y, x)
    tps = SIDE * SIDE

    for slot in (0, 1):
        for half in (0, 1):
            crossed(half, slot).wait_recv()
            cross(half, slot + 4).start()
    arrived[me] = outgo[me]

    @pl.loop(1, n_ep)
    def _(d):
        peer = lax.rem(me + d, n_ep)
        exchange_copy(outgo.at[0], arrived.at[peer], d_send, d_recv, me, peer, tp).wait_recv()

    for c in range(2):
        blocks = arrived[c * n_z : (c + 1) * n_z].reshape(part_slots, 128)
        xbuf[tp, c * part_rows : (c + 1) * part_rows, :] = jnp.dot(
            pack[...], blocks, preferred_element_type=F32
        ).astype(BF16)
    gather_x.begin()

    gather_x.relay_near()
    @pl.when(serving)
    def _():
        slices[me] = state[z]
        decays[me] = own_decay[0]

        @pl.loop(1, n_ep)
        def _(d):
            peer = lax.rem(me + d, n_ep)
            exchange_copy(state.at[0], slices.at[peer], s_send, s_recv, me, peer, tp).wait_recv()
            exchange_copy(own_decay.at[0], decays.at[peer], e_send, e_recv, me, peer, tp).wait_recv()

        total = jnp.zeros(slices.shape[1:], F32)
        for k in range(n_ep):
            prefix[k] = total
            total = decays[k] * total + slices[k]

        @pl.loop(1, n_ep)
        def _(d):
            peer = lax.rem(me + d, n_ep)
            exchange_copy(prefix.at[peer], incoming.at[z], p_send, p_recv, peer, z, tp).start()

        incoming[z] = prefix[me]

    gather_x.relay_far()
    gather_x.relay_last()
    loads["wg"].wait()
    loads["wu"].wait()
    feats = jnp.concatenate([xbuf[k] for k in range(tps)], axis=1)
    gate_act = jnp.dot(feats, wg_b[...], preferred_element_type=F32)
    up_act = jnp.dot(feats, wu_b[...], preferred_element_type=F32)
    hidden = (silu(gate_act) * up_act).astype(BF16)
    for c in range(2):
        hbuf[c, ring_g.pos(c)] = hidden[c * part_rows : (c + 1) * part_rows, :]

    first, last = pl.ds(0, part_rows // 2), pl.ds(part_rows // 2, part_rows // 2)

    def along(c, slot):
        block = hbuf.at[c, ring_g.pos(c, (0, 0, -1, 1)[slot])]
        block = block if slot < 2 else block.at[first if slot == 2 else last]
        return ring_g.copy(c, slot, block, block, (1, -1, 1, -1)[slot])

    def came_along(c, slot):
        block = hbuf.at[c, ring_g.pos(c, (-1, 1, 2, 2)[slot])]
        block = block if slot < 2 else block.at[first if slot == 2 else last]
        return ring_g.copy(c, slot, block, block, 1)

    for slot in (0, 1):
        for c in (0, 1):
            along(c, slot).start()
    for slot in (0, 1):
        for c in (0, 1):
            came_along(c, slot).wait_recv()
            along(c, slot + 2).start()

    @pl.loop(0, n_z)
    def _(k):
        @pl.when(2 * k + 1 != me)
        def _():
            exchange_copy(prefix.at[0], incoming.at[k], p_send, p_recv, me, k, tp).wait_recv()

    before_state = incoming[...].reshape(128, 128).astype(BF16)
    loads["og"].wait()
    loads["gain"].wait()
    out = local_out[...] + lax.dot_general(qdec[...], before_state, NT, preferred_element_type=F32)
    out = out * lax.rsqrt(jnp.mean(out * out, axis=1, keepdims=True) + EPS) * gain_b[...]
    mbuf[tp] = (out * silu(og_b[...].astype(F32))).astype(BF16)
    gather_m.begin()

    for copy in own_w:
        copy.wait()
    for slot in (2, 3, 4, 5):
        for c in (0, 1):
            crossed(c, slot).wait_recv()
    for slot in (2, 3):
        for c in (0, 1):
            came_along(c, slot).wait_recv()

    sums = ((2, first, 1), (2, last, -1), (1, last, 1), (-1, first, -1), (1, first, 1), (-1, last, -1))

    def across(c, slot):
        target, rows, way = sums[slot]
        return ring_r.copy(c, slot, sums_out.at[c, slot], sums_in.at[c, slot], way)

    for c in (0, 1):
        units = jnp.concatenate([hbuf[c, k] for k in range(SIDE)], axis=1)
        feats = jnp.concatenate([wcross[c, k].reshape(units.shape[1], 128) for k in range(SIDE)], axis=1)
        total = jnp.dot(units, feats, preferred_element_type=F32)
        for k in range(SIDE):
            part[c, k] = total[:, k * 128 : (k + 1) * 128]
        for slot in range(4):
            target, rows, _ = sums[slot]
            sums_out[c, slot] = part[c, ring_r.pos(c, target), rows, :].astype(BF16)
            across(c, slot).start()
    for slot in (0, 1):
        for c in (0, 1):
            across(c, slot).wait_recv()
            target, rows, _ = sums[slot + 4]
            sums_out[c, slot + 4] = (
                part[c, ring_r.pos(c, target), rows, :] + sums_in[c, slot].astype(F32)
            ).astype(BF16)
            across(c, slot + 4).start()
    gather_m.relay_first()
    for c in (0, 1):
        for slot in (2, 3, 4, 5):
            across(c, slot).wait_recv()
        mine = ring_r.pos(c)
        top = part[c, mine, first, :] + sums_in[c, 4].astype(F32) + sums_in[c, 3].astype(F32)
        low = part[c, mine, last, :] + sums_in[c, 2].astype(F32) + sums_in[c, 5].astype(F32)
        res = jnp.concatenate([top, low], axis=0).astype(BF16)
        result[c * n_z : (c + 1) * n_z] = (
            jnp.dot(spread[...], res, preferred_element_type=F32).astype(BF16).reshape(n_z, SLOT, 128)
        )

    for peer in peers:
        give_back(peer).start()

    returned[me] = result[me]
    gather_m.relay_second()
    gather_m.relay_far()
    gather_m.relay_last()
    loads["wout"].wait()
    heads = jnp.concatenate([mbuf[k] for k in range(tps)], axis=1)
    mixed_b[...] = jnp.dot(heads, wout_b[...], preferred_element_type=F32).astype(BF16)
    mixed_out = pltpu.make_async_copy(mixed_b, mixed_hbm, out_sem.at[0])
    mixed_out.start()

    for peer in peers:
        dispatch(peer).wait_send()
        give_back(peer).wait_send()

    @pl.when(serving)
    def _():
        @pl.loop(1, n_ep)
        def _(d):
            peer = lax.rem(me + d, n_ep)
            exchange_copy(prefix.at[peer], incoming.at[z], p_send, p_recv, peer, z, tp).wait_send()

    @pl.loop(0, n_z)
    def _(k):
        peer = 2 * k + 1

        @pl.when(peer != me)
        def _():
            exchange_copy(state.at[k], slices.at[me], s_send, s_recv, peer, me, tp).wait_send()
            exchange_copy(own_decay.at[0], decays.at[me], e_send, e_recv, peer, me, tp).wait_send()

    for gather in (gather_x, gather_m):
        gather.drain()
    for c in (0, 1):
        for slot in range(6):
            cross(c, slot).wait_send()
        for slot in range(4):
            along(c, slot).wait_send()
        for slot in range(6):
            across(c, slot).wait_send()
    @pl.loop(1, n_ep)
    def _(d):
        peer = lax.rem(me + d, n_ep)
        exchange_copy(result.at[0], returned.at[peer], c_send, c_recv, me, peer, tp).wait_recv()

    back = returned[...].reshape(n_ep * SLOT, 128)
    eout_b[...] = (
        jnp.dot(weights[0], back, preferred_element_type=F32) + jnp.dot(weights[1], back, preferred_element_type=F32)
    ).astype(BF16)
    expert_out = pltpu.make_async_copy(eout_b, eout_hbm, out_sem.at[1])
    expert_out.start()

    mixed_out.wait()
    expert_out.wait()


def solution(mesh):
    n_ep, n_tp = mesh.shape["ep"], mesh.shape["tp"]

    def local(q, fp, v, og, floor, surge, gain, wout, rows, ngain, grp, gex, cw, wg, wu, wd):
        length, count = q.shape[0], rows.shape[0]
        hid, cols = wg.shape[2], wd.shape[2]
        n_z, exp_rows = n_ep // 2, n_ep * CAP
        half_rows = exp_rows // 2
        anyspace = pl.BlockSpec(memory_space=pl.ANY)
        dma = pltpu.SemaphoreType.DMA
        operands = (
            q, fp, v, og, floor.reshape(1, -1), surge.reshape(-1, 128), gain.reshape(1, -1), wout,
            rows, ngain.reshape(1, -1), grp.reshape(1, -1), gex.T, cw.T, wg, wu, wd.reshape(SIDE, SIDE, hid, cols),
        )
        block = (n_ep, SLOT, 128)
        part = (n_ep, 128 // n_z, 128)
        outs = (jax.ShapeDtypeStruct((length, cols), BF16), jax.ShapeDtypeStruct((count, cols), BF16))
        scratch = [pltpu.VMEM(a.shape[1:] if a.ndim == 3 else a.shape, a.dtype) for a in (*operands, *outs)]
        scratch += [
            dma((len(operands),)), dma((2,)), dma((2,)),
            pltpu.VMEM(block, BF16), pltpu.VMEM(block, BF16), pltpu.VMEM(block, BF16), pltpu.VMEM(block, BF16),
            pltpu.VMEM((2, count, n_ep * SLOT), BF16),
            pltpu.VMEM((n_z * CAP, n_z * SLOT), BF16), pltpu.VMEM((n_z * SLOT, n_z * CAP), BF16),
            pltpu.VMEM((n_tp, exp_rows, 128), BF16), pltpu.VMEM((2, SIDE, half_rows, hid), BF16),
            pltpu.VMEM((n_tp, length, 128), BF16), pltpu.VMEM((2, SIDE, SIDE, hid, cols), BF16), pltpu.VMEM((2, 2, SIDE // 2, hid, cols), BF16),
            pltpu.VMEM((2, SIDE, half_rows, cols), F32),
            pltpu.VMEM((2, 6, half_rows // 2, cols), BF16), pltpu.VMEM((2, 6, half_rows // 2, cols), BF16),
            pltpu.VMEM(q.shape, F32), pltpu.VMEM(q.shape, F32), pltpu.VMEM(q.shape, F32), pltpu.VMEM(q.shape, BF16),
            pltpu.VMEM(q.shape, F32),
            pltpu.VMEM((n_z, *part[1:]), F32), pltpu.VMEM(part, F32),
            pltpu.VMEM((n_ep, 1, 128), F32), pltpu.VMEM((1, 1, 128), F32),
            pltpu.VMEM(part, F32), pltpu.VMEM((n_z, *part[1:]), F32),
        ]
        scratch += [dma((n_ep,))] * 10 + [dma((2, 20))] * 2 + [dma((2, 4))] * 2 + [dma((2, 20))] * 2 + [dma((2, 6))] * 2 + [dma((2, 6))] * 2
        return pl.pallas_call(
            functools.partial(kernel, n_ep),
            out_shape=outs,
            in_specs=[anyspace] * len(operands),
            out_specs=(anyspace, anyspace),
            scratch_shapes=scratch,
            compiler_params=pltpu.CompilerParams(
                collective_id=0, has_side_effects=True, vmem_limit_bytes=60 * 1024 * 1024
            ),
        )(*operands)

    return jax.shard_map(
        local,
        mesh=mesh,
        in_specs=(
            P("ep", "tp"), P("ep", "tp"), P("ep", "tp"), P("ep", "tp"), P("tp"), P("ep", "tp"), P(), P(None, "tp"),
            P("ep", None), P(), P("ep"), P("ep", None), P("ep", None),
            P("ep", None, "tp"), P("ep", None, "tp"), P("ep", None, "tp"),
        ),
        out_specs=(P("ep", "tp"), P("ep", "tp")),
        check_vma=False,
    )
```

```python
import functools

import jax
import jax.numpy as jnp
from jax import lax
from jax.experimental import pallas as pl
from jax.experimental.pallas import tpu as pltpu
from jax.sharding import PartitionSpec as P

MESH = pl.DeviceIdType.MESH
F32, BF16 = jnp.float32, jnp.bfloat16
EPS = 1e-06
GROUPS = 4
CAP = 12
SUB = 4
WIDE = CAP // SUB
SIDE = 4
NT = (((1,), (1,)), ((), ()))
OFFSETS = (0, -1, 1, 2)


def silu(v):
    return v / (1.0 + jnp.exp(-v))


class Gather:
    def __init__(self, buf, leap, send, recv, ep, y, x):
        self.buf, self.leap, self.rows = buf, leap, buf.shape[1]
        self.send, self.recv, self.ep, self.y, self.x = send, recv, ep, y, x

    def tp(self, color, a, b):
        dy, dx = (b, a) if color == 0 else (a, b)
        return lax.rem(self.y + dy + SIDE, SIDE) * SIDE + lax.rem(self.x + dx + SIDE, SIDE)

    def span(self, color, part):
        half = self.rows // 2
        start = color * half
        if part == 1:
            return pl.ds(start, half // 2)
        if part == 2:
            return pl.ds(start + half // 2, half // 2)
        return pl.ds(start, half)

    def copy(self, color, slot, block, part, to):
        region = self.buf.at[self.tp(color, *block), self.span(color, part), :]
        return pltpu.make_async_remote_copy(
            src_ref=region,
            dst_ref=region,
            send_sem=self.send.at[color, slot],
            recv_sem=self.recv.at[color, slot],
            device_id=(self.ep, self.tp(color, *to)),
            device_id_type=MESH,
        )

    def out(self, slot):
        if self.leap and slot == 2:
            return (0, 0), 0, (2, 0)
        if slot < 4:
            return [((0, 0), 0, (1, 0)), ((0, 0), 0, (-1, 0)), ((-1, 0), 1, (1, 0)), ((1, 0), 2, (-1, 0))][slot]
        j, k = divmod(slot - 4, 4)
        a = OFFSETS[j]
        return [((a, 0), 0, (0, 1)), ((a, 0), 0, (0, -1)), ((a, -1), 1, (0, 1)), ((a, 1), 2, (0, -1))][k]

    def landed(self, slot):
        if self.leap and slot == 2:
            return (2, 0), 0
        if slot < 4:
            return [((-1, 0), 0), ((1, 0), 0), ((2, 0), 1), ((2, 0), 2)][slot]
        j, k = divmod(slot - 4, 4)
        a = OFFSETS[j]
        return [((a, -1), 0), ((a, 1), 0), ((a, 2), 1), ((a, 2), 2)][k]

    def start(self, color, *slots):
        for slot in slots:
            self.copy(color, slot, *self.out(slot)).start()

    def arrive(self, color, *slots):
        for slot in slots:
            block, part = self.landed(slot)
            self.copy(color, slot, block, part, (1, 0)).wait_recv()

    def begin(self):
        for color in (0, 1):
            self.start(color, *((0, 1, 2) if self.leap else (0, 1)))
        for color in (0, 1):
            self.start(color, 4, 5)

    def relay(self):
        self.relay_sends()
        self.relay_last()

    def relay_sends(self):
        self.relay_near()
        self.relay_far()

    def relay_near(self):
        self.relay_first()
        self.opposite()
        self.relay_second()

    def relay_first(self):
        for k in (0, 1):
            for color in (0, 1):
                self.arrive(color, k)
                if not self.leap:
                    self.start(color, 2 + k)
                self.start(color, 4 + 4 * (k + 1), 5 + 4 * (k + 1))

    def relay_second(self):
        for color in (0, 1):
            self.arrive(color, 4)
            self.start(color, 6)
            self.arrive(color, 5)
            self.start(color, 7)

    def opposite(self):
        for color in (0, 1):
            self.arrive(color, *((2,) if self.leap else (2, 3)))
            self.start(color, 16, 17)

    def relay_far(self):
        for j in (1, 2, 3):
            for color in (0, 1):
                self.arrive(color, 4 + 4 * j)
                self.start(color, 6 + 4 * j)
                self.arrive(color, 5 + 4 * j)
                self.start(color, 7 + 4 * j)

    def relay_last(self):
        for j in (0, 1, 2, 3):
            for color in (0, 1):
                self.arrive(color, 6 + 4 * j, 7 + 4 * j)

    def drain(self):
        for color in (0, 1):
            for slot in range(20):
                if self.leap and slot == 3:
                    continue
                self.copy(color, slot, *self.out(slot)).wait_send()


class Ring:
    def __init__(self, turn, send, recv, ep, y, x):
        self.turn, self.send, self.recv, self.ep, self.y, self.x = turn, send, recv, ep, y, x

    def pos(self, half, off=0):
        return lax.rem((self.x if half == self.turn else self.y) + off + SIDE, SIDE)

    def tp(self, half, off):
        if half == self.turn:
            return self.y * SIDE + self.pos(half, off)
        return self.pos(half, off) * SIDE + self.x

    def copy(self, half, slot, src, dst, off):
        return pltpu.make_async_remote_copy(
            src_ref=src,
            dst_ref=dst,
            send_sem=self.send.at[half, slot],
            recv_sem=self.recv.at[half, slot],
            device_id=(self.ep, self.tp(half, off)),
            device_id_type=MESH,
        )


def exchange_copy(src, dst, send, recv, peer, mine, tp):
    return pltpu.make_async_remote_copy(
        src_ref=src,
        dst_ref=dst,
        send_sem=send.at[peer],
        recv_sem=recv.at[mine],
        device_id=(peer, tp),
        device_id_type=MESH,
    )


def kernel(
    n_ep,
    q_hbm, fp_hbm, v_hbm, og_hbm, floor_hbm, surge_hbm, gain_hbm, wout_hbm,
    rows_hbm, ngain_hbm, grp_hbm, gex_hbm, cw_hbm, wg_hbm, wu_hbm, wd_hbm,
    mixed_hbm, eout_hbm,
    q_b, fp_b, v_b, og_b, floor_b, surge_b, gain_b, wout_b,
    rows_b, ngain_b, grp_b, gex_b, cw_b, wg_b, wu_b, wd_b, mixed_b, eout_b, in_sem, out_sem, own_sem,
    outgo, arrived, result, returned, weights,
    xbuf, hbuf, mbuf, wcross, staged, wide, part, sums_out, sums_in,
    cum, keyin, qact, qdec, local_out,
    state, slices, decays, own_decay, prefix, incoming,
    d_send, d_recv, c_send, c_recv,
    s_send, s_recv, e_send, e_recv, p_send, p_recv,
    x_send, x_recv, h_send, h_recv, m_send, m_recv, w_send, w_recv, r_send, r_recv,
):
    me, tp = lax.axis_index("ep"), lax.axis_index("tp")
    y, x = lax.div(tp, SIDE), lax.rem(tp, SIDE)
    z, core = lax.div(me, 2), lax.rem(me, 2)
    n_z = n_ep // 2
    serving = core == 1

    loads = {}

    def load(*names):
        for name in names:
            loads[name].start()

    for k, (name, src, dst) in enumerate(
        (
            ("grp", grp_hbm, grp_b), ("gex", gex_hbm, gex_b), ("rows", rows_hbm, rows_b), ("ngain", ngain_hbm, ngain_b),
            ("wd", wd_hbm, wd_b), ("cw", cw_hbm, cw_b), ("floor", floor_hbm, floor_b), ("fp", fp_hbm, fp_b),
            ("surge", surge_hbm, surge_b), ("q", q_hbm, q_b), ("v", v_hbm, v_b), ("og", og_hbm, og_b),
            ("gain", gain_hbm, gain_b), ("wg", wg_hbm, wg_b), ("wu", wu_hbm, wu_b), ("wout", wout_hbm, wout_b),
        )
    ):
        loads[name] = pltpu.make_async_copy(src, dst, in_sem.at[k])
    load("grp", "gex", "rows", "ngain")

    order = [(n_z // 2, c) for c in (1, 0)]
    for away in range(n_z // 2 - 1, 0, -1):
        order += [(way * away, c) for c in (1, 0) for way in (1, -1)]
    order.append((0, 0))
    peers = [lax.rem(z + away + n_z, n_z) * 2 + lax.rem(core + c + 1, 2) for away, c in order]

    barrier = pltpu.get_barrier_semaphore()
    for peer in peers:
        pl.semaphore_signal(barrier, inc=1, device_id=(peer, tp), device_id_type=MESH)

    for dy, dx in ((0, 1), (0, -1), (1, 0), (-1, 0), (0, 2), (2, 0)):
        other = lax.rem(y + dy + SIDE, SIDE) * SIDE + lax.rem(x + dx + SIDE, SIDE)
        pl.semaphore_signal(barrier, inc=1, device_id=(me, other), device_id_type=MESH)

    load("wd", "floor", "fp", "surge", "q", "v", "cw", "og", "gain", "wg", "wu", "wout")

    loads["grp"].wait()
    loads["gex"].wait()
    count = grp_b.shape[1]
    per_group = n_ep // GROUPS
    ex0 = grp_b[...] * per_group + gex_b[0:1, :]
    ex1 = grp_b[...] * per_group + gex_b[1:2, :]
    e_iota = lax.broadcasted_iota(jnp.int32, (n_ep, count), 0)
    hit0, hit1 = (e_iota == ex0).astype(F32), (e_iota == ex1).astype(F32)
    before = lax.broadcasted_iota(jnp.int32, (count, count), 0) < lax.broadcasted_iota(jnp.int32, (count, count), 1)
    earlier = jnp.dot((hit0 + hit1).astype(BF16), before.astype(F32).astype(BF16), preferred_element_type=F32)
    slot0 = ex0 * CAP + jnp.sum(earlier * hit0, axis=0, keepdims=True).astype(jnp.int32)
    slot1 = ex1 * CAP + jnp.sum(earlier * hit1, axis=0, keepdims=True).astype(jnp.int32)
    s_iota = lax.broadcasted_iota(jnp.int32, (n_ep * SUB, count), 0)
    s_iota = s_iota // SUB * CAP + s_iota % SUB
    at0 = [s_iota + q * SUB == slot0 for q in range(WIDE)]
    at1 = [s_iota + q * SUB == slot1 for q in range(WIDE)]
    lanes = [slice(q * 128, q * 128 + 128) for q in range(WIDE)]

    loads["rows"].wait()
    loads["ngain"].wait()
    columns = pl.ds(pl.multiple_of(tp * 128, 128), 128)
    square = jnp.zeros((count, 128), F32)
    for k in range(rows_b.shape[1] // 128):
        piece = rows_b[:, k * 128 : (k + 1) * 128].astype(F32)
        square = square + piece * piece
    scale = lax.rsqrt(jnp.sum(square, axis=1, keepdims=True) * (1.0 / rows_b.shape[1]) + EPS)
    normed = (rows_b[:, columns].astype(F32) * scale * ngain_b[:, columns]).astype(BF16)
    for q in range(WIDE):
        place = jnp.where(at0[q] | at1[q], 1.0, 0.0).astype(BF16)
        block = jnp.dot(place, normed, preferred_element_type=F32).astype(BF16)
        outgo[:, :, lanes[q]] = block.reshape(n_ep, SUB, 128)

    pl.semaphore_wait(barrier, n_ep - 1 + 6)

    def dispatch(peer):
        return exchange_copy(outgo.at[peer], arrived.at[me], d_send, d_recv, peer, me, tp)

    def give_back(peer):
        return exchange_copy(result.at[peer], returned.at[me], c_send, c_recv, peer, me, tp)

    for peer in peers:
        dispatch(peer).start()

    loads["wd"].wait()
    ring_g = Ring(0, h_send, h_recv, me, y, x)
    ring_w = Ring(1, w_send, w_recv, me, y, x)
    ring_r = Ring(1, r_send, r_recv, me, y, x)

    def cross(half, slot):
        mine = ring_w.pos(half)

        def to(off, part):
            there = ring_w.pos(half, off)
            return wd_b.at[there, part] if half == 0 else wd_b.at[part, there]

        low, high = pl.ds(0, SIDE // 2), pl.ds(SIDE // 2, SIDE // 2)
        src, dst = (
            (lambda: to(2, low), lambda: staged.at[half, 0]),
            (lambda: to(2, high), lambda: staged.at[half, 1]),
            (lambda: to(1, low), lambda: wcross.at[half, mine, low]),
            (lambda: to(-1, low), lambda: wcross.at[half, mine, low]),
            (lambda: staged.at[half, 0], lambda: wcross.at[half, ring_w.pos(half, -1), low]),
            (lambda: staged.at[half, 1], lambda: wcross.at[half, ring_w.pos(half, 1), high]),
            (lambda: to(1, high), lambda: wcross.at[half, mine, high]),
            (lambda: to(-1, high), lambda: wcross.at[half, mine, high]),
        )[slot]
        return ring_w.copy(half, slot, src(), dst(), (1, -1)[slot % 2])

    def crossed(half, slot):
        low, high = pl.ds(0, SIDE // 2), pl.ds(SIDE // 2, SIDE // 2)
        region = (
            lambda: staged.at[half, 0],
            lambda: staged.at[half, 1],
            lambda: wcross.at[half, ring_w.pos(half, -1), low],
            lambda: wcross.at[half, ring_w.pos(half, 1), low],
            lambda: wcross.at[half, ring_w.pos(half, 2), low],
            lambda: wcross.at[half, ring_w.pos(half, 2), high],
            lambda: wcross.at[half, ring_w.pos(half, -1), high],
            lambda: wcross.at[half, ring_w.pos(half, 1), high],
        )[slot]()
        return ring_w.copy(half, slot, region, region, 1)

    for slot in range(4):
        for half in (0, 1):
            cross(half, slot).start()
    own_w = [
        pltpu.make_async_copy(wd_b.at[y], wcross.at[0, y], own_sem.at[0]),
        pltpu.make_async_copy(wd_b.at[:, x], wcross.at[1, x], own_sem.at[1]),
    ]
    for copy in own_w:
        copy.start()

    loads["floor"].wait()
    loads["fp"].wait()
    loads["surge"].wait()
    loads["q"].wait()
    loads["v"].wait()
    length = fp_b.shape[0]
    rate = jax.nn.sigmoid(-floor_b[...])
    lower = lax.broadcasted_iota(jnp.int32, (128, 128), 0) >= lax.broadcasted_iota(jnp.int32, (128, 128), 1)
    lower = jnp.where(lower, 1.0, 0.0)
    carry = jnp.zeros((1, 128), F32)
    for b in range(length // 128):
        r = slice(b * 128, b * 128 + 128)
        gate = rate * jax.nn.sigmoid(-fp_b[r, :].astype(F32))
        keyin[r, :] = gate
        total = jnp.dot(lower, jnp.log1p(-gate), precision=lax.Precision.HIGHEST, preferred_element_type=F32)
        total = total + jnp.sum(lower * surge_b[b : b + 1, :], axis=1, keepdims=True) + carry
        cum[r, :] = total
        carry = total[127:128, :]
        qact[r, :] = silu(q_b[r, :].astype(F32))

    own_decay[0] = jnp.exp(carry)
    tail = jnp.exp(carry - cum[...]) * keyin[...]
    state[...] = jnp.dot(v_b[...].astype(F32).T.astype(BF16), tail.astype(BF16), preferred_element_type=F32).reshape(
        state.shape
    )

    @pl.loop(0, n_z)
    def _(k):
        peer = 2 * k + 1

        @pl.when(peer != me)
        def _():
            exchange_copy(state.at[k], slices.at[me], s_send, s_recv, peer, me, tp).start()
            exchange_copy(own_decay.at[0], decays.at[me], e_send, e_recv, peer, me, tp).start()

    qdec[...] = (qact[...] * jnp.exp(cum[...])).astype(BF16)
    sub = 64

    @pl.loop(0, length // sub)
    def _(c):
        r = pl.ds(pl.multiple_of(c * sub, sub), sub)
        shape = (sub // 8, 8, 128)
        g, k, v = cum[r, :].reshape(shape), keyin[r, :].reshape(shape), v_b[r, :].astype(F32).reshape(shape)
        q = qact[r, :].reshape(shape)
        within = lax.broadcasted_iota(jnp.int32, (sub // 8, 8, 1), 1)
        total = jnp.sum(q * k, axis=2, keepdims=True) * v
        for d in range(1, 8):
            gd, kd, vd = (pltpu.roll(a, d, 1) for a in (g, k, v))
            w = jnp.sum(q * kd * jnp.exp(jnp.minimum(g - gd, 0.0)), axis=2, keepdims=True)
            total = total + jnp.where(within >= d, w, 0.0) * vd
        local_out[r, :] = total.reshape(sub, 128)

    half = length // 2
    t_iota = lax.broadcasted_iota(jnp.int32, (half, half), 0)
    u_iota = lax.broadcasted_iota(jnp.int32, (half, half), 1)
    for b in range(2):
        r = slice(b * half, (b + 1) * half)
        acc = jnp.zeros((half, half), F32)
        h = 8
        while h < half:
            g3 = cum[r, :].reshape(half // (2 * h), 2 * h, 128)
            fade = jnp.exp(-jnp.abs(g3 - g3[:, h - 1 : h, :])).reshape(half, 128)
            s = lax.dot_general(
                (qact[r, :] * fade).astype(BF16), (keyin[r, :] * fade).astype(BF16), NT, preferred_element_type=F32
            )
            pair = (t_iota // (2 * h) == u_iota // (2 * h)) & ((t_iota // h) % 2 == 1) & ((u_iota // h) % 2 == 0)
            acc = jnp.where(pair, s, acc)
            h *= 2
        local_out[r, :] += jnp.dot(acc.astype(BF16), v_b[r, :], preferred_element_type=F32)
    edge = cum[half - 1 : half, :]
    left, right = slice(0, half), slice(half, length)
    s = lax.dot_general(
        (qact[right, :] * jnp.exp(cum[right, :] - edge)).astype(BF16),
        (keyin[left, :] * jnp.exp(edge - cum[left, :])).astype(BF16),
        NT,
        preferred_element_type=F32,
    )
    local_out[right, :] += jnp.dot(s.astype(BF16), v_b[left, :], preferred_element_type=F32)

    part_rows = n_z * CAP
    loads["cw"].wait()
    for q in range(WIDE):
        chosen = jnp.where(at0[q], cw_b[0:1, :], 0.0) + jnp.where(at1[q], cw_b[1:2, :], 0.0)
        turned = chosen.T
        high = turned.astype(BF16)
        weights[0, :, lanes[q]] = high
        weights[1, :, lanes[q]] = (turned - high.astype(F32)).astype(BF16)

    gather_x = Gather(xbuf, True, x_send, x_recv, me, y, x)
    gather_m = Gather(mbuf, True, m_send, m_recv, me, y, x)
    tps = SIDE * SIDE

    for slot in (0, 1):
        for half in (0, 1):
            crossed(half, slot).wait_recv()
            cross(half, slot + 4).start()
    arrived[me] = outgo[me]

    @pl.loop(1, n_ep)
    def _(d):
        peer = lax.rem(me + d, n_ep)
        exchange_copy(outgo.at[0], arrived.at[peer], d_send, d_recv, me, peer, tp).wait_recv()

    share = n_z * SUB
    for c in range(2):
        for q in range(WIDE):
            start = c * part_rows + q * share
            xbuf[tp, start : start + share, :] = arrived[c * n_z : (c + 1) * n_z, :, lanes[q]].reshape(share, 128)
    gather_x.begin()

    gather_x.relay_near()
    @pl.when(serving)
    def _():
        slices[me] = state[z]
        decays[me] = own_decay[0]

        @pl.loop(1, n_ep)
        def _(d):
            peer = lax.rem(me + d, n_ep)
            exchange_copy(state.at[0], slices.at[peer], s_send, s_recv, me, peer, tp).wait_recv()
            exchange_copy(own_decay.at[0], decays.at[peer], e_send, e_recv, me, peer, tp).wait_recv()

        total = jnp.zeros(slices.shape[1:], F32)
        for k in range(n_ep):
            prefix[k] = total
            total = decays[k] * total + slices[k]

        @pl.loop(1, n_ep)
        def _(d):
            peer = lax.rem(me + d, n_ep)
            exchange_copy(prefix.at[peer], incoming.at[z], p_send, p_recv, peer, z, tp).start()

        incoming[z] = prefix[me]

    gather_x.relay_far()
    for slot in (6, 7):
        for half in (0, 1):
            cross(half, slot).start()
    loads["wg"].wait()
    loads["wu"].wait()

    def widen(c, off):
        at = lax.rem((y, x)[c] + off + SIDE, SIDE)
        r = slice(c * part_rows, (c + 1) * part_rows)
        if c == 0:
            feats = [xbuf[at * SIDE + k, r, :] for k in range(SIDE)]
            mats = [w[at].reshape(-1, w.shape[-1]) for w in (wg_b, wu_b)]
        else:
            feats = [xbuf[k * SIDE + at, r, :] for k in range(SIDE)]
            mats = [w[:, at].reshape(-1, w.shape[-1]) for w in (wg_b, wu_b)]
        feats = jnp.concatenate(feats, axis=1)
        return [jnp.dot(feats, w, preferred_element_type=F32) for w in mats]

    for c in (0, 1):
        pieces = [widen(c, off) for off in (0, -1, 1)]
        for k in (0, 1):
            wide[c, k] = pieces[0][k] + pieces[1][k] + pieces[2][k]
    gather_x.relay_last()
    for c in (0, 1):
        piece = widen(c, 2)
        hbuf[c, ring_g.pos(c)] = (silu(wide[c, 0] + piece[0]) * (wide[c, 1] + piece[1])).astype(BF16)

    ways = (2, 1, -1)

    def along(c, slot):
        block = hbuf.at[c, ring_g.pos(c)]
        return ring_g.copy(c, slot, block, block, ways[slot])

    def came_along(c, slot):
        block = hbuf.at[c, ring_g.pos(c, -ways[slot])]
        return ring_g.copy(c, slot, block, block, ways[slot])

    for slot in range(3):
        for c in (0, 1):
            along(c, slot).start()

    @pl.loop(0, n_z)
    def _(k):
        @pl.when(2 * k + 1 != me)
        def _():
            exchange_copy(prefix.at[0], incoming.at[k], p_send, p_recv, me, k, tp).wait_recv()

    before_state = incoming[...].reshape(128, 128).astype(BF16)
    loads["og"].wait()
    loads["gain"].wait()
    out = local_out[...] + lax.dot_general(qdec[...], before_state, NT, preferred_element_type=F32)
    out = out * lax.rsqrt(jnp.mean(out * out, axis=1, keepdims=True) + EPS) * gain_b[...]
    mbuf[tp] = (out * silu(og_b[...].astype(F32))).astype(BF16)

    gather_m.begin()
    for copy in own_w:
        copy.wait()
    for slot in (2, 3, 4, 5, 6, 7):
        for c in (0, 1):
            crossed(c, slot).wait_recv()

    def narrow(c, off):
        at = ring_g.pos(c, off)
        feats = jnp.concatenate([wcross[c, k, at] for k in range(SIDE)], axis=1)
        return jnp.dot(hbuf[c, at], feats, preferred_element_type=F32)

    for slot in (1, 2):
        for c in (0, 1):
            came_along(c, slot).wait_recv()
    for c in (0, 1):
        total = narrow(c, 0) + narrow(c, -1) + narrow(c, 1)
        for k in range(SIDE):
            part[c, k] = total[:, k * 128 : (k + 1) * 128]
    for c in (0, 1):
        came_along(c, 0).wait_recv()

    def across(c, slot):
        return ring_r.copy(c, slot, sums_out.at[c, slot], sums_in.at[c, slot], ways[slot])

    for c in (0, 1):
        total = narrow(c, 2)
        for k in range(SIDE):
            part[c, k] += total[:, k * 128 : (k + 1) * 128]
        for slot in range(3):
            sums_out[c, slot] = part[c, ring_r.pos(c, ways[slot])].astype(BF16)
            across(c, slot).start()
    gather_m.relay_first()
    gather_m.opposite()
    for c in (0, 1):
        for slot in (1, 2, 0):
            across(c, slot).wait_recv()
        res = part[c, ring_r.pos(c)]
        for slot in range(3):
            res = res + sums_in[c, slot].astype(F32)
        res = res.astype(BF16)
        for q in range(WIDE):
            rows = res[q * share : (q + 1) * share, :]
            result[c * n_z : (c + 1) * n_z, :, lanes[q]] = rows.reshape(n_z, SUB, 128)

    for peer in peers:
        give_back(peer).start()

    returned[me] = result[me]
    gather_m.relay_second()
    gather_m.relay_far()
    gather_m.relay_last()
    loads["wout"].wait()
    heads = jnp.concatenate([mbuf[k] for k in range(tps)], axis=1)
    mixed_b[...] = jnp.dot(heads, wout_b[...], preferred_element_type=F32).astype(BF16)
    mixed_out = pltpu.make_async_copy(mixed_b, mixed_hbm, out_sem.at[0])
    mixed_out.start()

    for peer in peers:
        dispatch(peer).wait_send()
        give_back(peer).wait_send()

    @pl.when(serving)
    def _():
        @pl.loop(1, n_ep)
        def _(d):
            peer = lax.rem(me + d, n_ep)
            exchange_copy(prefix.at[peer], incoming.at[z], p_send, p_recv, peer, z, tp).wait_send()

    @pl.loop(0, n_z)
    def _(k):
        peer = 2 * k + 1

        @pl.when(peer != me)
        def _():
            exchange_copy(state.at[k], slices.at[me], s_send, s_recv, peer, me, tp).wait_send()
            exchange_copy(own_decay.at[0], decays.at[me], e_send, e_recv, peer, me, tp).wait_send()

    for gather in (gather_x, gather_m):
        gather.drain()
    for c in (0, 1):
        for slot in range(8):
            cross(c, slot).wait_send()
        for slot in range(3):
            along(c, slot).wait_send()
            across(c, slot).wait_send()
    @pl.loop(1, n_ep)
    def _(d):
        peer = lax.rem(me + d, n_ep)
        exchange_copy(result.at[0], returned.at[peer], c_send, c_recv, me, peer, tp).wait_recv()

    back = jnp.concatenate([returned[:, :, lanes[q]].reshape(n_ep * SUB, 128) for q in range(WIDE)], axis=0)
    eout_b[...] = (
        jnp.dot(weights[0], back, preferred_element_type=F32) + jnp.dot(weights[1], back, preferred_element_type=F32)
    ).astype(BF16)
    expert_out = pltpu.make_async_copy(eout_b, eout_hbm, out_sem.at[1])
    expert_out.start()

    mixed_out.wait()
    expert_out.wait()


def solution(mesh):
    n_ep, n_tp = mesh.shape["ep"], mesh.shape["tp"]

    def local(q, fp, v, og, floor, surge, gain, wout, rows, ngain, grp, gex, cw, wg, wu, wd):
        length, count = q.shape[0], rows.shape[0]
        hid, cols = wg.shape[2], wd.shape[2]
        n_z, exp_rows = n_ep // 2, n_ep * CAP
        half_rows = exp_rows // 2
        anyspace = pl.BlockSpec(memory_space=pl.ANY)
        dma = pltpu.SemaphoreType.DMA
        operands = (
            q, fp, v, og, floor.reshape(1, -1), surge.reshape(-1, 128), gain.reshape(1, -1), wout,
            rows, ngain.reshape(1, -1), grp.reshape(1, -1), gex.T, cw.T,
            wg.reshape(SIDE, SIDE, 128, hid), wu.reshape(SIDE, SIDE, 128, hid), wd.reshape(SIDE, SIDE, hid, cols),
        )
        block = (n_ep, SUB, WIDE * 128)
        part = (n_ep, 128 // n_z, 128)
        outs = (jax.ShapeDtypeStruct((length, cols), BF16), jax.ShapeDtypeStruct((count, cols), BF16))
        scratch = [pltpu.VMEM(a.shape[1:] if a.ndim == 3 else a.shape, a.dtype) for a in (*operands, *outs)]
        scratch += [
            dma((len(operands),)), dma((2,)), dma((2,)),
            pltpu.VMEM(block, BF16), pltpu.VMEM(block, BF16), pltpu.VMEM(block, BF16), pltpu.VMEM(block, BF16),
            pltpu.VMEM((2, count, n_ep * CAP), BF16),
            pltpu.VMEM((n_tp, exp_rows, 128), BF16), pltpu.VMEM((2, SIDE, half_rows, hid), BF16),
            pltpu.VMEM((n_tp, length, 128), BF16), pltpu.VMEM((2, SIDE, SIDE, hid, cols), BF16), pltpu.VMEM((2, 2, SIDE // 2, hid, cols), BF16),
            pltpu.VMEM((2, 2, half_rows, hid), F32),
            pltpu.VMEM((2, SIDE, half_rows, cols), F32),
            pltpu.VMEM((2, 3, half_rows, cols), BF16), pltpu.VMEM((2, 3, half_rows, cols), BF16),
            pltpu.VMEM(q.shape, F32), pltpu.VMEM(q.shape, F32), pltpu.VMEM(q.shape, F32), pltpu.VMEM(q.shape, BF16),
            pltpu.VMEM(q.shape, F32),
            pltpu.VMEM((n_z, *part[1:]), F32), pltpu.VMEM(part, F32),
            pltpu.VMEM((n_ep, 1, 128), F32), pltpu.VMEM((1, 1, 128), F32),
            pltpu.VMEM(part, F32), pltpu.VMEM((n_z, *part[1:]), F32),
        ]
        scratch += [dma((n_ep,))] * 10 + [dma((2, 20))] * 2 + [dma((2, 3))] * 2 + [dma((2, 20))] * 2 + [dma((2, 8))] * 2 + [dma((2, 3))] * 2
        return pl.pallas_call(
            functools.partial(kernel, n_ep),
            out_shape=outs,
            in_specs=[anyspace] * len(operands),
            out_specs=(anyspace, anyspace),
            scratch_shapes=scratch,
            compiler_params=pltpu.CompilerParams(
                collective_id=0, has_side_effects=True, vmem_limit_bytes=60 * 1024 * 1024
            ),
        )(*operands)

    return jax.shard_map(
        local,
        mesh=mesh,
        in_specs=(
            P("ep", "tp"), P("ep", "tp"), P("ep", "tp"), P("ep", "tp"), P("tp"), P("ep", "tp"), P(), P(None, "tp"),
            P("ep", None), P(), P("ep"), P("ep", None), P("ep", None),
            P("ep", None, "tp"), P("ep", None, "tp"), P("ep", None, "tp"),
        ),
        out_specs=(P("ep", "tp"), P("ep", "tp")),
        check_vma=False,
    )
```

```python
import functools

import jax
import jax.numpy as jnp
from jax import lax
from jax.experimental import pallas as pl
from jax.experimental.pallas import tpu as pltpu
from jax.sharding import PartitionSpec as P

MESH = pl.DeviceIdType.MESH
F32, BF16 = jnp.float32, jnp.bfloat16
EPS = 1e-06
GROUPS = 4
CAP = 12
SUB = 4
WIDE = CAP // SUB
SIDE = 4
NT = (((1,), (1,)), ((), ()))
OFFSETS = (0, -1, 1, 2)


def silu(v):
    return v / (1.0 + jnp.exp(-v))


class Gather:
    def __init__(self, buf, leap, send, recv, ep, y, x):
        self.buf, self.leap, self.rows = buf, leap, buf.shape[1]
        self.send, self.recv, self.ep, self.y, self.x = send, recv, ep, y, x

    def tp(self, color, a, b):
        dy, dx = (b, a) if color == 0 else (a, b)
        return lax.rem(self.y + dy + SIDE, SIDE) * SIDE + lax.rem(self.x + dx + SIDE, SIDE)

    def span(self, color, part):
        half = self.rows // 2
        start = color * half
        if part == 1:
            return pl.ds(start, half // 2)
        if part == 2:
            return pl.ds(start + half // 2, half // 2)
        return pl.ds(start, half)

    def copy(self, color, slot, block, part, to):
        region = self.buf.at[self.tp(color, *block), self.span(color, part), :]
        return pltpu.make_async_remote_copy(
            src_ref=region,
            dst_ref=region,
            send_sem=self.send.at[color, slot],
            recv_sem=self.recv.at[color, slot],
            device_id=(self.ep, self.tp(color, *to)),
            device_id_type=MESH,
        )

    def out(self, slot):
        if self.leap and slot == 2:
            return (0, 0), 0, (2, 0)
        if slot < 4:
            return [((0, 0), 0, (1, 0)), ((0, 0), 0, (-1, 0)), ((-1, 0), 1, (1, 0)), ((1, 0), 2, (-1, 0))][slot]
        j, k = divmod(slot - 4, 4)
        a = OFFSETS[j]
        return [((a, 0), 0, (0, 1)), ((a, 0), 0, (0, -1)), ((a, -1), 1, (0, 1)), ((a, 1), 2, (0, -1))][k]

    def landed(self, slot):
        if self.leap and slot == 2:
            return (2, 0), 0
        if slot < 4:
            return [((-1, 0), 0), ((1, 0), 0), ((2, 0), 1), ((2, 0), 2)][slot]
        j, k = divmod(slot - 4, 4)
        a = OFFSETS[j]
        return [((a, -1), 0), ((a, 1), 0), ((a, 2), 1), ((a, 2), 2)][k]

    def start(self, color, *slots):
        for slot in slots:
            self.copy(color, slot, *self.out(slot)).start()

    def arrive(self, color, *slots):
        for slot in slots:
            block, part = self.landed(slot)
            self.copy(color, slot, block, part, (1, 0)).wait_recv()

    def begin(self):
        for color in (0, 1):
            self.start(color, *((0, 1, 2) if self.leap else (0, 1)))
        for color in (0, 1):
            self.start(color, 4, 5)

    def relay(self):
        self.relay_sends()
        self.relay_last()

    def relay_sends(self):
        self.relay_near()
        self.relay_far()

    def relay_near(self):
        self.relay_first()
        self.opposite()
        self.relay_second()

    def relay_first(self):
        for k in (0, 1):
            for color in (0, 1):
                self.arrive(color, k)
                if not self.leap:
                    self.start(color, 2 + k)
                self.start(color, 4 + 4 * (k + 1), 5 + 4 * (k + 1))

    def relay_second(self):
        for color in (0, 1):
            self.arrive(color, 4)
            self.start(color, 6)
            self.arrive(color, 5)
            self.start(color, 7)

    def opposite(self):
        for color in (0, 1):
            self.arrive(color, *((2,) if self.leap else (2, 3)))
            self.start(color, 16, 17)

    def relay_far(self):
        for j in (1, 2, 3):
            for color in (0, 1):
                self.arrive(color, 4 + 4 * j)
                self.start(color, 6 + 4 * j)
                self.arrive(color, 5 + 4 * j)
                self.start(color, 7 + 4 * j)

    def relay_last(self):
        for j in (0, 1, 2, 3):
            for color in (0, 1):
                self.arrive(color, 6 + 4 * j, 7 + 4 * j)

    def drain(self):
        for color in (0, 1):
            for slot in range(20):
                if self.leap and slot == 3:
                    continue
                self.copy(color, slot, *self.out(slot)).wait_send()


class Ring:
    def __init__(self, turn, send, recv, ep, y, x):
        self.turn, self.send, self.recv, self.ep, self.y, self.x = turn, send, recv, ep, y, x

    def pos(self, half, off=0):
        return lax.rem((self.x if half == self.turn else self.y) + off + SIDE, SIDE)

    def tp(self, half, off):
        if half == self.turn:
            return self.y * SIDE + self.pos(half, off)
        return self.pos(half, off) * SIDE + self.x

    def copy(self, half, slot, src, dst, off):
        return pltpu.make_async_remote_copy(
            src_ref=src,
            dst_ref=dst,
            send_sem=self.send.at[half, slot],
            recv_sem=self.recv.at[half, slot],
            device_id=(self.ep, self.tp(half, off)),
            device_id_type=MESH,
        )


def exchange_copy(src, dst, send, recv, peer, mine, tp):
    return pltpu.make_async_remote_copy(
        src_ref=src,
        dst_ref=dst,
        send_sem=send.at[peer],
        recv_sem=recv.at[mine],
        device_id=(peer, tp),
        device_id_type=MESH,
    )


def kernel(
    n_ep,
    q_hbm, fp_hbm, v_hbm, og_hbm, floor_hbm, surge_hbm, gain_hbm, wout_hbm,
    rows_hbm, ngain_hbm, grp_hbm, gex_hbm, cw_hbm, wg_hbm, wu_hbm, wd_hbm,
    mixed_hbm, eout_hbm,
    q_b, fp_b, v_b, og_b, floor_b, surge_b, gain_b, wout_b,
    rows_b, ngain_b, grp_b, gex_b, cw_b, wg_b, wu_b, wd_b, mixed_b, eout_b, in_sem, out_sem, own_sem,
    outgo, arrived, result, returned, weights,
    xbuf, hbuf, mbuf, wcross, staged, wide, part, sums_out, sums_in,
    cum, keyin, qact, qdec, local_out,
    state, slices, decays, own_decay, prefix, incoming,
    d_send, d_recv, c_send, c_recv,
    s_send, s_recv, e_send, e_recv, p_send, p_recv,
    x_send, x_recv, h_send, h_recv, m_send, m_recv, w_send, w_recv, r_send, r_recv,
):
    me, tp = lax.axis_index("ep"), lax.axis_index("tp")
    y, x = lax.div(tp, SIDE), lax.rem(tp, SIDE)
    z, core = lax.div(me, 2), lax.rem(me, 2)
    n_z = n_ep // 2
    serving = core == 1

    loads = {}

    def load(*names):
        for name in names:
            loads[name].start()

    for k, (name, src, dst) in enumerate(
        (
            ("grp", grp_hbm, grp_b), ("gex", gex_hbm, gex_b), ("rows", rows_hbm, rows_b), ("ngain", ngain_hbm, ngain_b),
            ("wd", wd_hbm, wd_b), ("cw", cw_hbm, cw_b), ("floor", floor_hbm, floor_b), ("fp", fp_hbm, fp_b),
            ("surge", surge_hbm, surge_b), ("q", q_hbm, q_b), ("v", v_hbm, v_b), ("og", og_hbm, og_b),
            ("gain", gain_hbm, gain_b), ("wg", wg_hbm, wg_b), ("wu", wu_hbm, wu_b), ("wout", wout_hbm, wout_b),
        )
    ):
        loads[name] = pltpu.make_async_copy(src, dst, in_sem.at[k])
    load("grp", "gex", "rows", "ngain")

    order = [(n_z // 2, c) for c in (1, 0)]
    for away in range(n_z // 2 - 1, 0, -1):
        order += [(way * away, c) for c in (1, 0) for way in (1, -1)]
    order.append((0, 0))
    peers = [lax.rem(z + away + n_z, n_z) * 2 + lax.rem(core + c + 1, 2) for away, c in order]

    barrier = pltpu.get_barrier_semaphore()
    for peer in peers:
        pl.semaphore_signal(barrier, inc=1, device_id=(peer, tp), device_id_type=MESH)

    for dy, dx in ((0, 1), (0, -1), (1, 0), (-1, 0), (0, 2), (2, 0)):
        other = lax.rem(y + dy + SIDE, SIDE) * SIDE + lax.rem(x + dx + SIDE, SIDE)
        pl.semaphore_signal(barrier, inc=1, device_id=(me, other), device_id_type=MESH)

    load("wd", "floor", "fp", "surge", "q", "v", "cw", "og", "gain", "wg", "wu", "wout")

    loads["grp"].wait()
    loads["gex"].wait()
    count = grp_b.shape[1]
    per_group = n_ep // GROUPS
    ex0 = grp_b[...] * per_group + gex_b[0:1, :]
    ex1 = grp_b[...] * per_group + gex_b[1:2, :]
    e_iota = lax.broadcasted_iota(jnp.int32, (n_ep, count), 0)
    hit0, hit1 = (e_iota == ex0).astype(F32), (e_iota == ex1).astype(F32)
    before = lax.broadcasted_iota(jnp.int32, (count, count), 0) < lax.broadcasted_iota(jnp.int32, (count, count), 1)
    earlier = jnp.dot((hit0 + hit1).astype(BF16), before.astype(F32).astype(BF16), preferred_element_type=F32)
    slot0 = ex0 * CAP + jnp.sum(earlier * hit0, axis=0, keepdims=True).astype(jnp.int32)
    slot1 = ex1 * CAP + jnp.sum(earlier * hit1, axis=0, keepdims=True).astype(jnp.int32)
    s_iota = lax.broadcasted_iota(jnp.int32, (n_ep * SUB, count), 0)
    s_iota = s_iota // SUB * CAP + s_iota % SUB
    at0 = [s_iota + q * SUB == slot0 for q in range(WIDE)]
    at1 = [s_iota + q * SUB == slot1 for q in range(WIDE)]
    lanes = [slice(q * 128, q * 128 + 128) for q in range(WIDE)]

    loads["rows"].wait()
    loads["ngain"].wait()
    columns = pl.ds(pl.multiple_of(tp * 128, 128), 128)
    square = jnp.zeros((count, 128), F32)
    for k in range(rows_b.shape[1] // 128):
        piece = rows_b[:, k * 128 : (k + 1) * 128].astype(F32)
        square = square + piece * piece
    scale = lax.rsqrt(jnp.sum(square, axis=1, keepdims=True) * (1.0 / rows_b.shape[1]) + EPS)
    normed = (rows_b[:, columns].astype(F32) * scale * ngain_b[:, columns]).astype(BF16)
    for q in range(WIDE):
        place = jnp.where(at0[q] | at1[q], 1.0, 0.0).astype(BF16)
        block = jnp.dot(place, normed, preferred_element_type=F32).astype(BF16)
        outgo[:, :, lanes[q]] = block.reshape(n_ep, SUB, 128)

    pl.semaphore_wait(barrier, n_ep - 1 + 6)

    def dispatch(peer):
        return exchange_copy(outgo.at[peer], arrived.at[me], d_send, d_recv, peer, me, tp)

    def give_back(peer):
        return exchange_copy(result.at[peer], returned.at[me], c_send, c_recv, peer, me, tp)

    for peer in peers:
        dispatch(peer).start()

    loads["wd"].wait()
    ring_g = Ring(0, h_send, h_recv, me, y, x)
    ring_w = Ring(1, w_send, w_recv, me, y, x)
    ring_r = Ring(1, r_send, r_recv, me, y, x)

    def cross(half, slot):
        mine = ring_w.pos(half)

        def to(off, part):
            there = ring_w.pos(half, off)
            return wd_b.at[there, part] if half == 0 else wd_b.at[part, there]

        low, high = pl.ds(0, SIDE // 2), pl.ds(SIDE // 2, SIDE // 2)
        src, dst = (
            (lambda: to(2, low), lambda: staged.at[half, 0]),
            (lambda: to(2, high), lambda: staged.at[half, 1]),
            (lambda: to(1, low), lambda: wcross.at[half, mine, low]),
            (lambda: to(-1, low), lambda: wcross.at[half, mine, low]),
            (lambda: staged.at[half, 0], lambda: wcross.at[half, ring_w.pos(half, -1), low]),
            (lambda: staged.at[half, 1], lambda: wcross.at[half, ring_w.pos(half, 1), high]),
            (lambda: to(1, high), lambda: wcross.at[half, mine, high]),
            (lambda: to(-1, high), lambda: wcross.at[half, mine, high]),
        )[slot]
        return ring_w.copy(half, slot, src(), dst(), (1, -1)[slot % 2])

    def crossed(half, slot):
        low, high = pl.ds(0, SIDE // 2), pl.ds(SIDE // 2, SIDE // 2)
        region = (
            lambda: staged.at[half, 0],
            lambda: staged.at[half, 1],
            lambda: wcross.at[half, ring_w.pos(half, -1), low],
            lambda: wcross.at[half, ring_w.pos(half, 1), low],
            lambda: wcross.at[half, ring_w.pos(half, 2), low],
            lambda: wcross.at[half, ring_w.pos(half, 2), high],
            lambda: wcross.at[half, ring_w.pos(half, -1), high],
            lambda: wcross.at[half, ring_w.pos(half, 1), high],
        )[slot]()
        return ring_w.copy(half, slot, region, region, 1)

    for slot in range(4):
        for half in (0, 1):
            cross(half, slot).start()
    own_w = [
        pltpu.make_async_copy(wd_b.at[y], wcross.at[0, y], own_sem.at[0]),
        pltpu.make_async_copy(wd_b.at[:, x], wcross.at[1, x], own_sem.at[1]),
    ]
    for copy in own_w:
        copy.start()

    loads["floor"].wait()
    loads["fp"].wait()
    loads["surge"].wait()
    loads["q"].wait()
    loads["v"].wait()
    length = fp_b.shape[0]
    rate = jax.nn.sigmoid(-floor_b[...])
    lower = lax.broadcasted_iota(jnp.int32, (128, 128), 0) >= lax.broadcasted_iota(jnp.int32, (128, 128), 1)
    lower = jnp.where(lower, 1.0, 0.0)
    carry = jnp.zeros((1, 128), F32)
    for b in range(length // 128):
        r = slice(b * 128, b * 128 + 128)
        gate = rate * jax.nn.sigmoid(-fp_b[r, :].astype(F32))
        keyin[r, :] = gate
        total = jnp.dot(lower, jnp.log1p(-gate), precision=lax.Precision.HIGHEST, preferred_element_type=F32)
        total = total + jnp.sum(lower * surge_b[b : b + 1, :], axis=1, keepdims=True) + carry
        cum[r, :] = total
        carry = total[127:128, :]
        qact[r, :] = silu(q_b[r, :].astype(F32))

    own_decay[0] = jnp.exp(carry)
    tail = jnp.exp(carry - cum[...]) * keyin[...]
    state[...] = jnp.dot(v_b[...].astype(F32).T.astype(BF16), tail.astype(BF16), preferred_element_type=F32).reshape(
        state.shape
    )

    @pl.loop(0, n_z)
    def _(k):
        peer = 2 * k + 1

        @pl.when(peer != me)
        def _():
            exchange_copy(state.at[k], slices.at[me], s_send, s_recv, peer, me, tp).start()
            exchange_copy(own_decay.at[0], decays.at[me], e_send, e_recv, peer, me, tp).start()

    qdec[...] = (qact[...] * jnp.exp(cum[...])).astype(BF16)
    sub = 64

    @pl.loop(0, length // sub)
    def _(c):
        r = pl.ds(pl.multiple_of(c * sub, sub), sub)
        shape = (sub // 8, 8, 128)
        g, k, v = cum[r, :].reshape(shape), keyin[r, :].reshape(shape), v_b[r, :].astype(F32).reshape(shape)
        q = qact[r, :].reshape(shape)
        within = lax.broadcasted_iota(jnp.int32, (sub // 8, 8, 1), 1)
        total = jnp.sum(q * k, axis=2, keepdims=True) * v
        for d in range(1, 8):
            gd, kd, vd = (pltpu.roll(a, d, 1) for a in (g, k, v))
            w = jnp.sum(q * kd * jnp.exp(jnp.minimum(g - gd, 0.0)), axis=2, keepdims=True)
            total = total + jnp.where(within >= d, w, 0.0) * vd
        local_out[r, :] = total.reshape(sub, 128)

    half = length // 2
    t_iota = lax.broadcasted_iota(jnp.int32, (half, half), 0)
    u_iota = lax.broadcasted_iota(jnp.int32, (half, half), 1)
    for b in range(2):
        r = slice(b * half, (b + 1) * half)
        acc = jnp.zeros((half, half), F32)
        h = 8
        while h < half:
            g3 = cum[r, :].reshape(half // (2 * h), 2 * h, 128)
            fade = jnp.exp(-jnp.abs(g3 - g3[:, h - 1 : h, :])).reshape(half, 128)
            s = lax.dot_general(
                (qact[r, :] * fade).astype(BF16), (keyin[r, :] * fade).astype(BF16), NT, preferred_element_type=F32
            )
            pair = (t_iota // (2 * h) == u_iota // (2 * h)) & ((t_iota // h) % 2 == 1) & ((u_iota // h) % 2 == 0)
            acc = jnp.where(pair, s, acc)
            h *= 2
        local_out[r, :] += jnp.dot(acc.astype(BF16), v_b[r, :], preferred_element_type=F32)
    edge = cum[half - 1 : half, :]
    left, right = slice(0, half), slice(half, length)
    s = lax.dot_general(
        (qact[right, :] * jnp.exp(cum[right, :] - edge)).astype(BF16),
        (keyin[left, :] * jnp.exp(edge - cum[left, :])).astype(BF16),
        NT,
        preferred_element_type=F32,
    )
    local_out[right, :] += jnp.dot(s.astype(BF16), v_b[left, :], preferred_element_type=F32)

    part_rows = n_z * CAP
    loads["cw"].wait()
    for q in range(WIDE):
        chosen = jnp.where(at0[q], cw_b[0:1, :], 0.0) + jnp.where(at1[q], cw_b[1:2, :], 0.0)
        turned = chosen.T
        high = turned.astype(BF16)
        weights[0, :, lanes[q]] = high
        weights[1, :, lanes[q]] = (turned - high.astype(F32)).astype(BF16)

    gather_x = Gather(xbuf, True, x_send, x_recv, me, y, x)
    gather_m = Gather(mbuf, True, m_send, m_recv, me, y, x)
    tps = SIDE * SIDE

    for slot in (0, 1):
        for half in (0, 1):
            crossed(half, slot).wait_recv()
            cross(half, slot + 4).start()
    arrived[me] = outgo[me]

    @pl.loop(1, n_ep)
    def _(d):
        peer = lax.rem(me + d, n_ep)
        exchange_copy(outgo.at[0], arrived.at[peer], d_send, d_recv, me, peer, tp).wait_recv()

    share = n_z * SUB
    for c in range(2):
        for q in range(WIDE):
            start = c * part_rows + q * share
            xbuf[tp, start : start + share, :] = arrived[c * n_z : (c + 1) * n_z, :, lanes[q]].reshape(share, 128)
    gather_x.begin()

    gather_x.relay_near()
    @pl.when(serving)
    def _():
        slices[me] = state[z]
        decays[me] = own_decay[0]

        @pl.loop(1, n_ep)
        def _(d):
            peer = lax.rem(me + d, n_ep)
            exchange_copy(state.at[0], slices.at[peer], s_send, s_recv, me, peer, tp).wait_recv()
            exchange_copy(own_decay.at[0], decays.at[peer], e_send, e_recv, me, peer, tp).wait_recv()

        total = jnp.zeros(slices.shape[1:], F32)
        for k in range(n_ep):
            prefix[k] = total.astype(BF16)
            total = decays[k] * total + slices[k]

        for peer in peers:
            exchange_copy(prefix.at[peer], incoming.at[z], p_send, p_recv, peer, z, tp).start()

        incoming[z] = prefix[me]

    gather_x.relay_far()
    for slot in (6, 7):
        for half in (0, 1):
            cross(half, slot).start()
    loads["wg"].wait()
    loads["wu"].wait()

    def widen(c, off):
        at = lax.rem((y, x)[c] + off + SIDE, SIDE)
        r = slice(c * part_rows, (c + 1) * part_rows)
        if c == 0:
            feats = [xbuf[at * SIDE + k, r, :] for k in range(SIDE)]
            mats = [w[at].reshape(-1, w.shape[-1]) for w in (wg_b, wu_b)]
        else:
            feats = [xbuf[k * SIDE + at, r, :] for k in range(SIDE)]
            mats = [w[:, at].reshape(-1, w.shape[-1]) for w in (wg_b, wu_b)]
        feats = jnp.concatenate(feats, axis=1)
        return [jnp.dot(feats, w, preferred_element_type=F32) for w in mats]

    for c in (0, 1):
        pieces = [widen(c, off) for off in (0, -1, 1)]
        for k in (0, 1):
            wide[c, k] = pieces[0][k] + pieces[1][k] + pieces[2][k]
    gather_x.relay_last()
    ways = (2, 1, -1)

    def along(c, slot):
        block = hbuf.at[c, ring_g.pos(c)]
        return ring_g.copy(c, slot, block, block, ways[slot])

    def came_along(c, slot):
        block = hbuf.at[c, ring_g.pos(c, -ways[slot])]
        return ring_g.copy(c, slot, block, block, ways[slot])

    for c in (0, 1):
        piece = widen(c, 2)
        hbuf[c, ring_g.pos(c)] = (silu(wide[c, 0] + piece[0]) * (wide[c, 1] + piece[1])).astype(BF16)
        for slot in range(3):
            along(c, slot).start()

    @pl.loop(0, n_z)
    def _(k):
        @pl.when(2 * k + 1 != me)
        def _():
            exchange_copy(prefix.at[0], incoming.at[k], p_send, p_recv, me, k, tp).wait_recv()

    before_state = incoming[...].reshape(128, 128)
    loads["og"].wait()
    loads["gain"].wait()
    out = local_out[...] + lax.dot_general(qdec[...], before_state, NT, preferred_element_type=F32)
    out = out * lax.rsqrt(jnp.mean(out * out, axis=1, keepdims=True) + EPS) * gain_b[...]
    mbuf[tp] = (out * silu(og_b[...].astype(F32))).astype(BF16)

    gather_m.begin()
    for copy in own_w:
        copy.wait()
    for slot in (2, 3, 4, 5, 6, 7):
        for c in (0, 1):
            crossed(c, slot).wait_recv()

    def narrow(c, off):
        at = ring_g.pos(c, off)
        feats = jnp.concatenate([wcross[c, k, at] for k in range(SIDE)], axis=1)
        return jnp.dot(hbuf[c, at], feats, preferred_element_type=F32)

    for slot in (1, 2):
        for c in (0, 1):
            came_along(c, slot).wait_recv()
    for c in (0, 1):
        total = narrow(c, 0) + narrow(c, -1) + narrow(c, 1)
        for k in range(SIDE):
            part[c, k] = total[:, k * 128 : (k + 1) * 128]
    for c in (0, 1):
        came_along(c, 0).wait_recv()

    def across(c, slot):
        return ring_r.copy(c, slot, sums_out.at[c, slot], sums_in.at[c, slot], ways[slot])

    for c in (0, 1):
        total = narrow(c, 2)
        for k in range(SIDE):
            part[c, k] += total[:, k * 128 : (k + 1) * 128]
        for slot in range(3):
            sums_out[c, slot] = part[c, ring_r.pos(c, ways[slot])].astype(BF16)
            across(c, slot).start()
    gather_m.relay_first()
    gather_m.opposite()
    for c in (0, 1):
        for slot in (1, 2, 0):
            across(c, slot).wait_recv()
        res = part[c, ring_r.pos(c)]
        for slot in range(3):
            res = res + sums_in[c, slot].astype(F32)
        res = res.astype(BF16)
        for q in range(WIDE):
            rows = res[q * share : (q + 1) * share, :]
            result[c * n_z : (c + 1) * n_z, :, lanes[q]] = rows.reshape(n_z, SUB, 128)

    for peer in peers:
        give_back(peer).start()

    returned[me] = result[me]
    gather_m.relay_second()
    gather_m.relay_far()
    gather_m.relay_last()
    loads["wout"].wait()
    heads = jnp.concatenate([mbuf[k] for k in range(tps)], axis=1)
    mixed_b[...] = jnp.dot(heads, wout_b[...], preferred_element_type=F32).astype(BF16)
    mixed_out = pltpu.make_async_copy(mixed_b, mixed_hbm, out_sem.at[0])
    mixed_out.start()

    for peer in peers:
        dispatch(peer).wait_send()
        give_back(peer).wait_send()

    @pl.when(serving)
    def _():
        @pl.loop(1, n_ep)
        def _(d):
            peer = lax.rem(me + d, n_ep)
            exchange_copy(prefix.at[peer], incoming.at[z], p_send, p_recv, peer, z, tp).wait_send()

    @pl.loop(0, n_z)
    def _(k):
        peer = 2 * k + 1

        @pl.when(peer != me)
        def _():
            exchange_copy(state.at[k], slices.at[me], s_send, s_recv, peer, me, tp).wait_send()
            exchange_copy(own_decay.at[0], decays.at[me], e_send, e_recv, peer, me, tp).wait_send()

    for gather in (gather_x, gather_m):
        gather.drain()
    for c in (0, 1):
        for slot in range(8):
            cross(c, slot).wait_send()
        for slot in range(3):
            along(c, slot).wait_send()
            across(c, slot).wait_send()
    @pl.loop(1, n_ep)
    def _(d):
        peer = lax.rem(me + d, n_ep)
        exchange_copy(result.at[0], returned.at[peer], c_send, c_recv, me, peer, tp).wait_recv()

    back = jnp.concatenate([returned[:, :, lanes[q]].reshape(n_ep * SUB, 128) for q in range(WIDE)], axis=0)
    eout_b[...] = (
        jnp.dot(weights[0], back, preferred_element_type=F32) + jnp.dot(weights[1], back, preferred_element_type=F32)
    ).astype(BF16)
    expert_out = pltpu.make_async_copy(eout_b, eout_hbm, out_sem.at[1])
    expert_out.start()

    mixed_out.wait()
    expert_out.wait()


def solution(mesh):
    n_ep, n_tp = mesh.shape["ep"], mesh.shape["tp"]

    def local(q, fp, v, og, floor, surge, gain, wout, rows, ngain, grp, gex, cw, wg, wu, wd):
        length, count = q.shape[0], rows.shape[0]
        hid, cols = wg.shape[2], wd.shape[2]
        n_z, exp_rows = n_ep // 2, n_ep * CAP
        half_rows = exp_rows // 2
        anyspace = pl.BlockSpec(memory_space=pl.ANY)
        dma = pltpu.SemaphoreType.DMA
        operands = (
            q, fp, v, og, floor.reshape(1, -1), surge.reshape(-1, 128), gain.reshape(1, -1), wout,
            rows, ngain.reshape(1, -1), grp.reshape(1, -1), gex.T, cw.T,
            wg.reshape(SIDE, SIDE, 128, hid), wu.reshape(SIDE, SIDE, 128, hid), wd.reshape(SIDE, SIDE, hid, cols),
        )
        block = (n_ep, SUB, WIDE * 128)
        part = (n_ep, 128 // n_z, 128)
        outs = (jax.ShapeDtypeStruct((length, cols), BF16), jax.ShapeDtypeStruct((count, cols), BF16))
        scratch = [pltpu.VMEM(a.shape[1:] if a.ndim == 3 else a.shape, a.dtype) for a in (*operands, *outs)]
        scratch += [
            dma((len(operands),)), dma((2,)), dma((2,)),
            pltpu.VMEM(block, BF16), pltpu.VMEM(block, BF16), pltpu.VMEM(block, BF16), pltpu.VMEM(block, BF16),
            pltpu.VMEM((2, count, n_ep * CAP), BF16),
            pltpu.VMEM((n_tp, exp_rows, 128), BF16), pltpu.VMEM((2, SIDE, half_rows, hid), BF16),
            pltpu.VMEM((n_tp, length, 128), BF16), pltpu.VMEM((2, SIDE, SIDE, hid, cols), BF16), pltpu.VMEM((2, 2, SIDE // 2, hid, cols), BF16),
            pltpu.VMEM((2, 2, half_rows, hid), F32),
            pltpu.VMEM((2, SIDE, half_rows, cols), F32),
            pltpu.VMEM((2, 3, half_rows, cols), BF16), pltpu.VMEM((2, 3, half_rows, cols), BF16),
            pltpu.VMEM(q.shape, F32), pltpu.VMEM(q.shape, F32), pltpu.VMEM(q.shape, F32), pltpu.VMEM(q.shape, BF16),
            pltpu.VMEM(q.shape, F32),
            pltpu.VMEM((n_z, *part[1:]), F32), pltpu.VMEM(part, F32),
            pltpu.VMEM((n_ep, 1, 128), F32), pltpu.VMEM((1, 1, 128), F32),
            pltpu.VMEM(part, BF16), pltpu.VMEM((n_z, *part[1:]), BF16),
        ]
        scratch += [dma((n_ep,))] * 10 + [dma((2, 20))] * 2 + [dma((2, 3))] * 2 + [dma((2, 20))] * 2 + [dma((2, 8))] * 2 + [dma((2, 3))] * 2
        return pl.pallas_call(
            functools.partial(kernel, n_ep),
            out_shape=outs,
            in_specs=[anyspace] * len(operands),
            out_specs=(anyspace, anyspace),
            scratch_shapes=scratch,
            compiler_params=pltpu.CompilerParams(
                collective_id=0, has_side_effects=True, vmem_limit_bytes=60 * 1024 * 1024
            ),
        )(*operands)

    return jax.shard_map(
        local,
        mesh=mesh,
        in_specs=(
            P("ep", "tp"), P("ep", "tp"), P("ep", "tp"), P("ep", "tp"), P("tp"), P("ep", "tp"), P(), P(None, "tp"),
            P("ep", None), P(), P("ep"), P("ep", None), P("ep", None),
            P("ep", None, "tp"), P("ep", None, "tp"), P("ep", None, "tp"),
        ),
        out_specs=(P("ep", "tp"), P("ep", "tp")),
        check_vma=False,
    )
```
